32 devices in a mesh: fs: 4 (over y, x), tp: 8 (over z, core).
Axes of the slice: x: 2, y: 2, z: 4, core: 2. Of those that a mesh axis runs over, the one named last changes fastest.
Arguments:
- tokens: bfloat16 [4096, 2048], P(('fs', 'tp')), may hold values from -6 to 6
- gate_weight: bfloat16 [2048, 5632], P('fs', 'tp'), may hold values from -0.125 to 0.125
- up_weight: bfloat16 [2048, 5632], P('fs', 'tp'), may hold values from -0.125 to 0.125
- down_weight: bfloat16 [5632, 2048], P('tp', 'fs'), may hold values from -0.078125 to 0.078125
- grad_out: bfloat16 [4096, 2048], P(('fs', 'tp')), may hold values from -6 to 6
Outputs:
- grad_input: bfloat16 [4096, 2048], P(('fs', 'tp'))
- grad_gate: float32 [2048, 5632], P('fs', 'tp')
- grad_up: float32 [2048, 5632], P('fs', 'tp')
- grad_down: float32 [5632, 2048], P('tp', 'fs')
The draws below stay inside these ranges and needn't reach their ends.
All inputs are finite; a program needn't handle non-finite values.
Results may differ from the reference program's by a relative error of at most 0.0049.
Values may be sent and summed in bfloat16 or wider, within the bound.
A program may use at most 128 MiB of HBM per device.

```python
import jax
import jax.numpy as jnp

D = 2048
FF = 5632
TOKENS = 4096


def spiked(array, key, source, target, parts, factor):
    owner, partner = [(jnp.arange(array.shape[dim]) // (array.shape[dim] // parts)).reshape([-1 if axis == dim else 1 for axis in range(array.ndim)]) for dim in (source, target)]
    chosen = jax.random.permutation(key, parts)[partner]
    strong = (owner == chosen) | (owner == (partner + parts // 2) % parts)
    return jnp.where(strong, factor * array, array)


def shard_levels(own_key, dims, shards, least, high):
    factor_of, own = 1.0, jax.random.fold_in(own_key, 6)
    for position, shards_of in shards:
        draws = jnp.exp(jax.random.uniform(jax.random.fold_in(own, position), (shards_of,), jnp.float32, least / len(shards), high / len(shards)))
        factor_of = factor_of * jnp.repeat(draws, dims[position] // shards_of).reshape([-1 if axis == position else 1 for axis in range(len(dims))])
    return factor_of


def bell_draw(own_key, dims, spread, limit, split=(), held_as=jnp.bfloat16):
    factor_of = shard_levels(own_key, dims, split, -0.22, 0.18) if split else 1.0
    result = jax.random.normal(own_key, dims, jnp.float32) * spread * factor_of
    return jnp.minimum(jnp.maximum(result, -limit), limit).astype(held_as)


def gaussian_with(key, extent, width, bound, shards, heavy, held_as=jnp.bfloat16):
    entries = width * jax.random.normal(key, extent, jnp.float32)
    if shards:
        entries = entries * shard_levels(key, extent, shards, -0.22, 0.18)
    return jnp.clip(spiked(entries, jax.random.fold_in(key, 3), *heavy), -bound, bound).astype(held_as)


def setup_inputs(seed: int = 0) -> dict:
    splits = jax.random.split(jax.random.key(seed), 6)
    tokens = bell_draw(splits[0], (TOKENS, D), 1.0, 6.0, ((0, 32),))
    gate_weight = bell_draw(splits[1], (D, FF), D ** -0.5, 0.125, ((0, 4), (1, 8)))
    up_weight = bell_draw(splits[2], (D, FF), D ** -0.5, 0.125, ((0, 4), (1, 8)))
    down_weight = bell_draw(splits[3], (FF, D), FF ** -0.5, 0.078125, ((0, 8), (1, 4)))
    grad_out = gaussian_with(splits[4], (TOKENS, D), 1.0, 6.0, ((0, 32),), (0, 1, 32, 2.75))
    return {"tokens": tokens, "gate_weight": gate_weight, "up_weight": up_weight, "down_weight": down_weight, "grad_out": grad_out}


def reference(tokens, gate_weight, up_weight, down_weight, grad_out):
    gate_pre = jnp.dot(tokens, gate_weight, preferred_element_type=jnp.float32)
    up_pre = jnp.dot(tokens, up_weight, preferred_element_type=jnp.float32)
    sig_gate = jax.nn.sigmoid(gate_pre)
    active = gate_pre * sig_gate
    hidden = (active * up_pre).astype(jnp.bfloat16)
    d_hidden = jnp.dot(grad_out, down_weight.T, preferred_element_type=jnp.float32)
    d_gate = (d_hidden * up_pre * sig_gate * (1.0 + gate_pre * (1.0 - sig_gate))).astype(jnp.bfloat16)
    d_up = (d_hidden * active).astype(jnp.bfloat16)
    grad_input = (jnp.dot(d_gate, gate_weight.T, preferred_element_type=jnp.float32)
                  + jnp.dot(d_up, up_weight.T, preferred_element_type=jnp.float32)).astype(jnp.bfloat16)
    grad_gate = jnp.dot(tokens.T, d_gate, preferred_element_type=jnp.float32)
    grad_up = jnp.dot(tokens.T, d_up, preferred_element_type=jnp.float32)
    grad_down = jnp.dot(hidden.T, grad_out, preferred_element_type=jnp.float32)
    return grad_input, grad_gate, grad_up, grad_down
```

```python
import functools

import jax
import jax.numpy as jnp
from jax import lax
from jax.experimental import pallas as pl
from jax.experimental.pallas import tpu as pltpu
from jax.sharding import PartitionSpec as P

MESH = pl.DeviceIdType.MESH
CORES = 2
PARTS = 2
F32 = jnp.float32


def nt(left, right):
    return lax.dot_general(left, right, (((1,), (1,)), ((), ())), preferred_element_type=F32)


def nn(left, right):
    return jnp.dot(left, right, preferred_element_type=F32)


def orders_of(n_fs):
    bits = [1 << i for i in range(n_fs.bit_length() - 1)]
    return (bits, bits[::-1])


def first_bit(order, mask):
    return next(i for i, bit in enumerate(order) if mask & bit)


def compact(order, mask):
    return sum(1 << i for i, bit in enumerate(order) if mask & bit)


def greet(n_fs, depth, fs, tp, z):
    barrier = pltpu.get_barrier_semaphore()
    bits = orders_of(n_fs)[0]

    def hello(fs_id, tp_id):
        pl.semaphore_signal(barrier, inc=1, device_id=(fs_id, tp_id), device_id_type=MESH)

    for bit in bits:
        hello(fs ^ bit, tp)
    hello(fs, tp ^ 1)

    @pl.when(z > 0)
    def _():
        hello(fs, tp - CORES)

    @pl.when(z < depth - 1)
    def _():
        hello(fs, tp + CORES)

    ends = (z > 0).astype(jnp.int32) + (z < depth - 1).astype(jnp.int32)
    pl.semaphore_wait(barrier, len(bits) + 1 + ends)


def layer_kernel(n_fs, n_tp, *refs):
    ins, outs, scratch = refs[:5], refs[5:9], refs[9:]
    tok_all, cot_all, gate_full, up_full, down_full = scratch[:5]
    act_buf, fac_buf, hid_t, dgate_t, dup_t, dgate, dup = scratch[5:12]
    grads, recvs, stages, w_res = scratch[12:15], scratch[15:18], scratch[18:21], scratch[21:24]
    gi, c_buf, z_buf, gi_res = scratch[24:28]
    gw_send, gw_recv, gz_send, gz_recv, gc_send, gc_recv, l_sem = scratch[28:35]
    sw_send, sw_recv, sz_send, sz_recv, sc_send, sc_recv, o_sem = scratch[35:]
    fs, tp = lax.axis_index("fs"), lax.axis_index("tp")
    depth = n_tp // CORES
    z, core = tp // CORES, tp % CORES
    orders = orders_of(n_fs)
    phases = len(orders[0])
    bf16 = tok_all.dtype
    rows_all, width = tok_all.shape
    n = rows_all // n_tp
    ff = gate_full.shape[0]
    cols = width // n_fs
    half = ff // 2
    sub = n // PARTS
    rows = (tok_all, cot_all)
    weights = (gate_full, up_full, down_full)

    def slab(owner):
        return pl.ds(pl.multiple_of(owner * cols, cols), cols)

    def own_rows(owner):
        return pl.ds(pl.multiple_of(owner * n, n), n)

    local = [
        pltpu.make_async_copy(ins[0], tok_all.at[own_rows(tp), :], l_sem.at[0]),
        pltpu.make_async_copy(ins[1], gate_full.at[:, slab(fs)], l_sem.at[1]),
        pltpu.make_async_copy(ins[2], up_full.at[:, slab(fs)], l_sem.at[2]),
        pltpu.make_async_copy(ins[3], down_full.at[:, slab(fs)], l_sem.at[3]),
        pltpu.make_async_copy(ins[4], cot_all.at[own_rows(tp), :], l_sem.at[4]),
    ]
    for copy in local:
        copy.start()
    greet(n_fs, depth, fs, tp, z)
    for copy in local:
        copy.wait()

    def gw_copy(array, split, phase, mask):
        order = orders[split]
        there = weights[array].at[pl.ds(split * half, half), slab(fs ^ mask)]
        slot = (array, split, (1 << phase) - 1 + sum(1 << i for i in range(phase) if mask & order[i]))
        return pltpu.make_async_remote_copy(
            src_ref=there,
            dst_ref=there,
            send_sem=gw_send.at[slot],
            recv_sem=gw_recv.at[slot],
            device_id=(fs ^ order[phase], tp),
            device_id_type=MESH,
        )

    def gw_start(array):
        for phase in range(phases):
            for split in range(2):
                gw_copy(array, split, phase, 0).start()

    def gw_event(array, phase, index):
        for split in range(2):
            order = orders[split]
            mask = sum(order[i] for i in range(phase) if index & (1 << i))
            gw_copy(array, split, phase, mask).wait_recv()
            got = mask | order[phase]
            for later in range(phase + 1, phases):
                gw_copy(array, split, later, got).start()

    def gw_relays(array):
        for phase in range(phases - 1):
            for index in range(1 << phase):
                gw_event(array, phase, index)

    def gw_finish(array):
        for index in range(1 << (phases - 1)):
            gw_event(array, phases - 1, index)

    def r_block(array, owner, part):
        start = pl.multiple_of(owner * n + part * sub, sub)
        return rows[array].at[pl.ds(start, sub), :]

    def gz_copy(array, way, step, part):
        sign = 1 if way == 0 else -1
        there = r_block(array, tp - sign * step * CORES, part)
        slot = (array, way, step, part)
        return pltpu.make_async_remote_copy(
            src_ref=there,
            dst_ref=there,
            send_sem=gz_send.at[slot],
            recv_sem=gz_recv.at[slot],
            device_id=(fs, tp + sign * CORES),
            device_id_type=MESH,
        )

    def g_sends(way, step):
        if way == 0:
            return jnp.logical_and(z - step >= 0, z < depth - 1)
        return jnp.logical_and(z + step <= depth - 1, z > 0)

    def g_arrives(way, step):
        return z - 1 - step >= 0 if way == 0 else z + 1 + step <= depth - 1

    def gc_copy(array, way, step, part):
        sign = 1 if way == 0 else -1
        there = r_block(array, tp - sign * (step + 1) * CORES, part)
        slot = (array, way, step + 1, part)
        return pltpu.make_async_remote_copy(
            src_ref=there,
            dst_ref=there,
            send_sem=gc_send.at[slot],
            recv_sem=gc_recv.at[slot],
            device_id=(fs, tp ^ 1),
            device_id_type=MESH,
        )

    def gz_start(array):
        for part in range(PARTS):
            for way in range(2):

                @pl.when(g_sends(way, 0))
                def _():
                    gz_copy(array, way, 0, part).start()

            gc_copy(array, 0, -1, part).start()

    def gz_event(array, step, part):
        for way in range(2):

            @pl.when(g_arrives(way, step))
            def _():
                gz_copy(array, way, step, part).wait_recv()

            if step + 1 < depth - 1:

                @pl.when(g_sends(way, step + 1))
                def _():
                    gz_copy(array, way, step + 1, part).start()

            @pl.when(g_arrives(way, step))
            def _():
                gc_copy(array, way, step, part).start()

    def gz_events(array, first, last):
        for step in range(first, last):
            for part in range(PARTS):
                gz_event(array, step, part)

    def gc_finish(array):
        for part in range(PARTS):
            gc_copy(array, 0, -1, part).wait_recv()
            for way in range(2):
                for step in range(depth - 1):

                    @pl.when(g_arrives(way, step))
                    def _():
                        gc_copy(array, way, step, part).wait_recv()

    def sw_own(array, split, mask):
        return grads[array].at[pl.ds(split * half, half), slab(fs ^ mask)]

    def sw_copy(array, split, mask):
        order = orders[split]
        phase = first_bit(order, mask)
        slot = compact(order, mask) - 1
        src = sw_own(array, split, mask) if phase == 0 else stages[array].at[split, slot // 2]
        return pltpu.make_async_remote_copy(
            src_ref=src,
            dst_ref=recvs[array].at[split, slot],
            send_sem=sw_send.at[array, split, slot],
            recv_sem=sw_recv.at[array, split, slot],
            device_id=(fs ^ order[phase], tp),
            device_id_type=MESH,
        )

    def sw_sum(array, split, mask):
        order = orders[split]
        total = sw_own(array, split, mask)[...].astype(F32)
        limit = phases if mask == 0 else first_bit(order, mask)
        for phase in range(limit):
            sent = mask | order[phase]
            sw_copy(array, split, sent).wait_recv()
            total += recvs[array][split, compact(order, sent) - 1].astype(F32)
        return total

    later = [m for m in range(1, n_fs) if not m & 1]
    later = sorted(later, key=lambda m: ((m & -m), -m))

    def sw_relay(array):
        for mask in later:
            for split in range(2):
                order = orders[split]
                real = sum(bit for i, bit in enumerate(order) if mask & (1 << i))
                slot = mask - 1
                stages[array][split, slot // 2] = sw_sum(array, split, real).astype(bf16)
                sw_copy(array, split, real).start()

    def sw_finish(array):
        for split in range(2):
            w_res[array][pl.ds(split * half, half), :] = sw_sum(array, split, 0)
        pltpu.make_async_copy(w_res[array], outs[1 + array], o_sem.at[1 + array]).start()

    firsts = (orders[0][0], orders[1][0])
    masks = sorted(
        range(n_fs), key=lambda m: (-sum(1 for b in firsts if m & b), -m)
    )

    def weight_grad(array, left, right):
        for mask in masks:
            grads[array][:, slab(fs ^ mask)] = nn(left[...], right[:, slab(fs ^ mask)]).astype(bf16)
            for split in range(2):
                if mask & firsts[split]:
                    sw_copy(array, split, mask).start()

    def g_rows(target, which, part):
        start = (target * CORES + which) * n + part * sub
        return pl.ds(pl.multiple_of(start, sub), sub)

    def sc_copy(target, part):
        return pltpu.make_async_remote_copy(
            src_ref=gi.at[g_rows(target, 1 - core, part), :],
            dst_ref=c_buf.at[target, part],
            send_sem=sc_send.at[target, part],
            recv_sem=sc_recv.at[target, part],
            device_id=(fs, tp ^ 1),
            device_id_type=MESH,
        )

    def z_target(way, step):
        return depth - 1 - step if way == 0 else step

    def sz_copy(way, step, part):
        return pltpu.make_async_remote_copy(
            src_ref=c_buf.at[z_target(way, step), part],
            dst_ref=z_buf.at[way, step, part],
            send_sem=sz_send.at[way, step, part],
            recv_sem=sz_recv.at[way, step, part],
            device_id=(fs, tp + CORES if way == 0 else tp - CORES),
            device_id_type=MESH,
        )

    def s_sends(way, step):
        t = z_target(way, step)
        return t > z if way == 0 else t < z

    def s_arrives(way, step):
        t = z_target(way, step)
        return jnp.logical_and(z > 0, t >= z) if way == 0 else jnp.logical_and(z < depth - 1, t <= z)

    targets = [depth - 1 - i // 2 if i % 2 == 0 else i // 2 for i in range(depth)]

    def sc_event(t):
        for part in range(PARTS):
            sc_copy(t, part).wait_recv()
            c_buf[t, part] = (
                c_buf[t, part].astype(F32) + gi[g_rows(t, core, part), :].astype(F32)
            ).astype(bf16)

    def sz_event(step):
        for part in range(PARTS):
            for way in range(2):
                t = z_target(way, step)

                @pl.when(s_arrives(way, step))
                def _():
                    sz_copy(way, step, part).wait_recv()

                @pl.when(s_sends(way, step))
                def _():
                    @pl.when(s_arrives(way, step))
                    def _():
                        c_buf[t, part] = (
                            c_buf[t, part].astype(F32) + z_buf[way, step, part].astype(F32)
                        ).astype(bf16)

                    sz_copy(way, step, part).start()

    def sz_finish():
        zero = jnp.zeros((sub, width), F32)
        for part in range(PARTS):
            total = c_buf[z, part].astype(F32)
            from_left = z_buf[0, jnp.clip(depth - 1 - z, 0, depth - 2), part].astype(F32)
            from_right = z_buf[1, jnp.clip(z, 0, depth - 2), part].astype(F32)
            total += jnp.where(z > 0, from_left, zero)
            total += jnp.where(z < depth - 1, from_right, zero)
            gi_res[pl.ds(part * sub, sub), :] = total.astype(bf16)
        pltpu.make_async_copy(gi_res, outs[0], o_sem.at[0]).start()

    tile = min(256, rows_all)

    def over_tiles(step):
        def run(i, carry):
            step(pl.ds(pl.multiple_of(i * tile, tile), tile))
            return carry

        lax.fori_loop(0, rows_all // tile, run, 0)

    def gate_step(at):
        act_buf[:, at] = nt(gate_full[...], tok_all[at, :])

    def up_step(at):
        up_pre = nt(up_full[...], tok_all[at, :])
        gate_pre = act_buf[:, at]
        sig = jax.nn.sigmoid(gate_pre)
        active = gate_pre * sig
        hid_t[:, at] = (active * up_pre).astype(bf16)
        act_buf[:, at] = active
        fac_buf[:, at] = up_pre * sig * (1.0 + gate_pre * (1.0 - sig))

    def down_step(at):
        d_hidden = nt(down_full[...], cot_all[at, :])
        d_gate = d_hidden * fac_buf[:, at]
        d_up = d_hidden * act_buf[:, at]
        dgate_t[:, at] = d_gate.astype(bf16)
        dup_t[:, at] = d_up.astype(bf16)
        dgate[at, :] = d_gate.T.astype(bf16)
        dup[at, :] = d_up.T.astype(bf16)

    gi_tile = min(512, width)

    def gi_steps(first, last):
        def run(i, carry):
            at = pl.ds(pl.multiple_of(i * gi_tile, gi_tile), gi_tile)
            gi[:, at] = (nn(dgate[...], gate_full[:, at]) + nn(dup[...], up_full[:, at])).astype(bf16)
            return carry

        lax.fori_loop(first, last, run, 0)

    TOK, COT = 0, 1
    GATE, UP, DOWN = 0, 1, 2

    gz_start(TOK)
    gw_start(GATE)
    gz_event(TOK, 0, 0)
    gw_relays(GATE)
    gw_start(UP)
    for part in range(1, PARTS):
        gz_event(TOK, 0, part)
    gz_events(TOK, 1, depth - 2)
    gz_start(COT)
    gw_finish(GATE)
    gz_event(TOK, depth - 2, 0)
    gw_relays(UP)
    gw_start(DOWN)
    for part in range(1, PARTS):
        gz_event(TOK, depth - 2, part)
    gc_finish(TOK)
    over_tiles(gate_step)
    gz_events(COT, 0, 1)
    gw_finish(UP)
    over_tiles(up_step)
    gz_events(COT, 1, depth - 2)
    gw_relays(DOWN)
    gz_events(COT, depth - 2, depth - 1)
    gc_finish(COT)
    weight_grad(2, hid_t, cot_all)
    gw_finish(DOWN)
    over_tiles(down_step)
    gi_count = width // gi_tile
    gi_steps(0, gi_count // 2)
    sw_relay(2)
    gi_steps(gi_count // 2, gi_count)
    for t in targets:
        for part in range(PARTS):
            sc_copy(t, part).start()
    weight_grad(0, dgate_t, tok_all)
    for t in targets:
        sc_event(t)
    sz_event(0)
    weight_grad(1, dup_t, tok_all)
    for step in range(1, depth - 2):
        sz_event(step)
    sw_relay(0)
    sw_finish(2)
    for step in range(max(depth - 2, 1), depth - 1):
        sz_event(step)
    sw_relay(1)
    sz_finish()
    sw_finish(0)
    sw_finish(1)

    for array in range(2):
        for part in range(PARTS):
            gc_copy(array, 0, -1, part).wait_send()
            for way in range(2):
                for step in range(depth - 1):

                    @pl.when(g_sends(way, step))
                    def _():
                        gz_copy(array, way, step, part).wait_send()

                    @pl.when(g_arrives(way, step))
                    def _():
                        gc_copy(array, way, step, part).wait_send()

    for array in range(3):
        for split in range(2):
            order = orders[split]
            for phase in range(phases):
                for index in range(1 << phase):
                    mask = sum(order[i] for i in range(phase) if index & (1 << i))
                    gw_copy(array, split, phase, mask).wait_send()
            for mask in range(1, n_fs):
                sw_copy(array, split, mask).wait_send()

    for part in range(PARTS):
        for t in targets:
            sc_copy(t, part).wait_send()
        for way in range(2):
            for step in range(depth - 1):

                @pl.when(s_sends(way, step))
                def _():
                    sz_copy(way, step, part).wait_send()

    pltpu.make_async_copy(gi_res, outs[0], o_sem.at[0]).wait()
    for array in range(3):
        pltpu.make_async_copy(w_res[array], outs[1 + array], o_sem.at[1 + array]).wait()


def layer(n_fs, n_tp, tokens, gate, up, down, cot):
    depth = n_tp // CORES
    n, width = tokens.shape
    ff, cols = gate.shape
    rows_all = n * n_tp
    bf16 = tokens.dtype
    hbm = pl.BlockSpec(memory_space=pl.ANY)
    vmem = pltpu.VMEM
    dma = pltpu.SemaphoreType.DMA
    half, sub = ff // 2, n // PARTS
    n_stage = max(n_fs // 2 - 1, 1)
    scratch = (
        [vmem((rows_all, width), bf16)] * 2
        + [vmem((ff, width), bf16)] * 3
        + [vmem((ff, rows_all), F32)] * 2
        + [vmem((ff, rows_all), bf16)] * 3
        + [vmem((rows_all, ff), bf16)] * 2
        + [vmem((ff, width), bf16)] * 3
        + [vmem((2, n_fs - 1, half, cols), bf16)] * 3
        + [vmem((2, n_stage, half, cols), bf16)] * 3
        + [vmem((ff, cols), F32)] * 3
        + [
            vmem((rows_all, width), bf16),
            vmem((depth, PARTS, sub, width), bf16),
            vmem((2, depth - 1, PARTS, sub, width), bf16),
            vmem((n, width), bf16),
        ]
        + [
            dma((3, 2, n_fs - 1)),
            dma((3, 2, n_fs - 1)),
            dma((2, 2, depth - 1, PARTS)),
            dma((2, 2, depth - 1, PARTS)),
            dma((2, 2, depth, PARTS)),
            dma((2, 2, depth, PARTS)),
            dma((5,)),
            dma((3, 2, n_fs - 1)),
            dma((3, 2, n_fs - 1)),
            dma((2, depth - 1, PARTS)),
            dma((2, depth - 1, PARTS)),
            dma((depth, PARTS)),
            dma((depth, PARTS)),
            dma((4,)),
        ]
    )
    return pl.pallas_call(
        functools.partial(layer_kernel, n_fs, n_tp),
        out_shape=(jax.ShapeDtypeStruct((n, width), bf16),)
        + tuple(jax.ShapeDtypeStruct((ff, cols), F32) for _ in range(3)),
        in_specs=[hbm] * 5,
        out_specs=[hbm] * 4,
        scratch_shapes=scratch,
        compiler_params=pltpu.CompilerParams(
            collective_id=0, has_side_effects=True, vmem_limit_bytes=67043328
        ),
        name="layer",
    )(tokens, gate, up, down, cot)


def body(n_fs, n_tp, tokens, gate_weight, up_weight, down_weight, grad_out):
    grad_input, grad_gate, grad_up, grad_down = layer(
        n_fs, n_tp, tokens, gate_weight.T, up_weight.T, down_weight, grad_out
    )
    return grad_input, grad_gate.T, grad_up.T, grad_down


def solution(mesh):
    in_specs = (
        P(("fs", "tp"), None),
        P("fs", "tp"),
        P("fs", "tp"),
        P("tp", "fs"),
        P(("fs", "tp"), None),
    )
    out_specs = (P(("fs", "tp"), None), P("fs", "tp"), P("fs", "tp"), P("tp", "fs"))
    return jax.shard_map(
        functools.partial(body, mesh.shape["fs"], mesh.shape["tp"]),
        mesh=mesh,
        in_specs=in_specs,
        out_specs=out_specs,
        check_vma=False,
    )
```

```python
import functools

import jax
import jax.numpy as jnp
from jax import lax
from jax.experimental import pallas as pl
from jax.experimental.pallas import tpu as pltpu
from jax.sharding import PartitionSpec as P

MESH = pl.DeviceIdType.MESH
CORES = 2
PARTS = 2
F32 = jnp.float32


def nt(left, right):
    return lax.dot_general(left, right, (((1,), (1,)), ((), ())), preferred_element_type=F32)


def nn(left, right):
    return jnp.dot(left, right, preferred_element_type=F32)


def orders_of(n_fs):
    bits = [1 << i for i in range(n_fs.bit_length() - 1)]
    return (bits, bits[::-1])


def first_bit(order, mask):
    return next(i for i, bit in enumerate(order) if mask & bit)


def compact(order, mask):
    return sum(1 << i for i, bit in enumerate(order) if mask & bit)


def greet(n_fs, depth, fs, tp, z):
    barrier = pltpu.get_barrier_semaphore()
    bits = orders_of(n_fs)[0]

    def hello(fs_id, tp_id):
        pl.semaphore_signal(barrier, inc=1, device_id=(fs_id, tp_id), device_id_type=MESH)

    for bit in bits:
        hello(fs ^ bit, tp)
    hello(fs, tp ^ 1)

    @pl.when(z > 0)
    def _():
        hello(fs, tp - CORES)

    @pl.when(z < depth - 1)
    def _():
        hello(fs, tp + CORES)

    ends = (z > 0).astype(jnp.int32) + (z < depth - 1).astype(jnp.int32)
    pl.semaphore_wait(barrier, len(bits) + 1 + ends)


def layer_kernel(n_fs, n_tp, *refs):
    ins, outs, scratch = refs[:5], refs[5:9], refs[9:]
    tok_all, cot_all, gate_full, up_full, down_full = scratch[:5]
    act_buf, fac_buf, hid_t, dgate_t, dup_t, dgate, dup = scratch[5:12]
    grads, recvs, stages, w_res = scratch[12:15], scratch[15:18], scratch[18:21], scratch[21:24]
    gi, c_buf, z_buf, gi_res = scratch[24:28]
    gw_send, gw_recv, gz_send, gz_recv, gc_send, gc_recv, l_sem = scratch[28:35]
    sw_send, sw_recv, sz_send, sz_recv, sc_send, sc_recv, o_sem = scratch[35:]
    fs, tp = lax.axis_index("fs"), lax.axis_index("tp")
    depth = n_tp // CORES
    z, core = tp // CORES, tp % CORES
    orders = orders_of(n_fs)
    phases = len(orders[0])
    bf16 = tok_all.dtype
    rows_all, width = tok_all.shape
    n = rows_all // n_tp
    ff = gate_full.shape[0]
    cols = width // n_fs
    half = ff // 2
    sub = n // PARTS
    rows = (tok_all, cot_all)
    weights = (gate_full, up_full, down_full)

    def slab(owner):
        return pl.ds(pl.multiple_of(owner * cols, cols), cols)

    def own_rows(owner):
        return pl.ds(pl.multiple_of(owner * n, n), n)

    local = [
        pltpu.make_async_copy(ins[0], tok_all.at[own_rows(tp), :], l_sem.at[0]),
        pltpu.make_async_copy(ins[1], gate_full.at[:, slab(fs)], l_sem.at[1]),
        pltpu.make_async_copy(ins[2], up_full.at[:, slab(fs)], l_sem.at[2]),
        pltpu.make_async_copy(ins[3], down_full.at[:, slab(fs)], l_sem.at[3]),
        pltpu.make_async_copy(ins[4], cot_all.at[own_rows(tp), :], l_sem.at[4]),
    ]
    for copy in local:
        copy.start()
    greet(n_fs, depth, fs, tp, z)
    for copy in local:
        copy.wait()

    def gw_copy(array, split, phase, mask):
        order = orders[split]
        there = weights[array].at[pl.ds(split * half, half), slab(fs ^ mask)]
        slot = (array, split, (1 << phase) - 1 + sum(1 << i for i in range(phase) if mask & order[i]))
        return pltpu.make_async_remote_copy(
            src_ref=there,
            dst_ref=there,
            send_sem=gw_send.at[slot],
            recv_sem=gw_recv.at[slot],
            device_id=(fs ^ order[phase], tp),
            device_id_type=MESH,
        )

    def gw_start(array):
        for phase in range(phases):
            for split in range(2):
                gw_copy(array, split, phase, 0).start()

    def gw_event(array, phase, index):
        for split in range(2):
            order = orders[split]
            mask = sum(order[i] for i in range(phase) if index & (1 << i))
            gw_copy(array, split, phase, mask).wait_recv()
            got = mask | order[phase]
            for later in range(phase + 1, phases):
                gw_copy(array, split, later, got).start()

    def gw_relays(array):
        for phase in range(phases - 1):
            for index in range(1 << phase):
                gw_event(array, phase, index)

    def gw_finish(array):
        for index in range(1 << (phases - 1)):
            gw_event(array, phases - 1, index)

    def r_block(array, owner, part):
        start = pl.multiple_of(owner * n + part * sub, sub)
        return rows[array].at[pl.ds(start, sub), :]

    def gz_copy(array, way, step, part):
        sign = 1 if way == 0 else -1
        there = r_block(array, tp - sign * step * CORES, part)
        slot = (array, way, step, part)
        return pltpu.make_async_remote_copy(
            src_ref=there,
            dst_ref=there,
            send_sem=gz_send.at[slot],
            recv_sem=gz_recv.at[slot],
            device_id=(fs, tp + sign * CORES),
            device_id_type=MESH,
        )

    def g_sends(way, step):
        if way == 0:
            return jnp.logical_and(z - step >= 0, z < depth - 1)
        return jnp.logical_and(z + step <= depth - 1, z > 0)

    def g_arrives(way, step):
        return z - 1 - step >= 0 if way == 0 else z + 1 + step <= depth - 1

    def gc_copy(array, way, step, part):
        sign = 1 if way == 0 else -1
        there = r_block(array, tp - sign * (step + 1) * CORES, part)
        slot = (array, way, step + 1, part)
        return pltpu.make_async_remote_copy(
            src_ref=there,
            dst_ref=there,
            send_sem=gc_send.at[slot],
            recv_sem=gc_recv.at[slot],
            device_id=(fs, tp ^ 1),
            device_id_type=MESH,
        )

    def gz_start(array):
        for part in range(PARTS):
            for way in range(2):

                @pl.when(g_sends(way, 0))
                def _():
                    gz_copy(array, way, 0, part).start()

            gc_copy(array, 0, -1, part).start()

    def gz_event(array, step, part):
        for way in range(2):

            @pl.when(g_arrives(way, step))
            def _():
                gz_copy(array, way, step, part).wait_recv()

            if step + 1 < depth - 1:

                @pl.when(g_sends(way, step + 1))
                def _():
                    gz_copy(array, way, step + 1, part).start()

            @pl.when(g_arrives(way, step))
            def _():
                gc_copy(array, way, step, part).start()

    def gz_events(array, first, last):
        for step in range(first, last):
            for part in range(PARTS):
                gz_event(array, step, part)

    def gc_finish(array):
        for part in range(PARTS):
            gc_copy(array, 0, -1, part).wait_recv()
            for way in range(2):
                for step in range(depth - 1):

                    @pl.when(g_arrives(way, step))
                    def _():
                        gc_copy(array, way, step, part).wait_recv()

    def sw_own(array, split, mask):
        return grads[array].at[pl.ds(split * half, half), slab(fs ^ mask)]

    def sw_copy(array, split, mask):
        order = orders[split]
        phase = first_bit(order, mask)
        slot = compact(order, mask) - 1
        src = sw_own(array, split, mask) if phase == 0 else stages[array].at[split, slot // 2]
        return pltpu.make_async_remote_copy(
            src_ref=src,
            dst_ref=recvs[array].at[split, slot],
            send_sem=sw_send.at[array, split, slot],
            recv_sem=sw_recv.at[array, split, slot],
            device_id=(fs ^ order[phase], tp),
            device_id_type=MESH,
        )

    def sw_sum(array, split, mask):
        order = orders[split]
        total = sw_own(array, split, mask)[...].astype(F32)
        limit = phases if mask == 0 else first_bit(order, mask)
        for phase in range(limit):
            sent = mask | order[phase]
            sw_copy(array, split, sent).wait_recv()
            total += recvs[array][split, compact(order, sent) - 1].astype(F32)
        return total

    later = [m for m in range(1, n_fs) if not m & 1]
    later = sorted(later, key=lambda m: ((m & -m), -m))

    def sw_relay(array):
        for mask in later:
            for split in range(2):
                order = orders[split]
                real = sum(bit for i, bit in enumerate(order) if mask & (1 << i))
                slot = mask - 1
                stages[array][split, slot // 2] = sw_sum(array, split, real).astype(bf16)
                sw_copy(array, split, real).start()

    def sw_finish(array):
        for split in range(2):
            w_res[array][pl.ds(split * half, half), :] = sw_sum(array, split, 0)
        pltpu.make_async_copy(w_res[array], outs[1 + array], o_sem.at[1 + array]).start()

    firsts = (orders[0][0], orders[1][0])
    masks = sorted(
        range(n_fs), key=lambda m: (-sum(1 for b in firsts if m & b), -m)
    )

    def weight_grad(array, left, right):
        for mask in masks:
            grads[array][:, slab(fs ^ mask)] = nn(left[...], right[:, slab(fs ^ mask)]).astype(bf16)
            for split in range(2):
                if mask & firsts[split]:
                    sw_copy(array, split, mask).start()

    def g_rows(target, which, part):
        start = (target * CORES + which) * n + part * sub
        return pl.ds(pl.multiple_of(start, sub), sub)

    def sc_copy(target, part):
        return pltpu.make_async_remote_copy(
            src_ref=gi.at[g_rows(target, 1 - core, part), :],
            dst_ref=c_buf.at[target, part],
            send_sem=sc_send.at[target, part],
            recv_sem=sc_recv.at[target, part],
            device_id=(fs, tp ^ 1),
            device_id_type=MESH,
        )

    def sz_from(way):
        return z if way == 0 else depth - 1 - z

    def sz_target(way, step):
        return depth - 1 - step if way == 0 else step

    def sz_copy(way, step, part):
        return pltpu.make_async_remote_copy(
            src_ref=c_buf.at[sz_target(way, step), part],
            dst_ref=z_buf.at[way, step, part],
            send_sem=sz_send.at[way, step, part],
            recv_sem=sz_recv.at[way, step, part],
            device_id=(fs, tp + CORES if way == 0 else tp - CORES),
            device_id_type=MESH,
        )

    def s_sends(way, step):
        return step < depth - 1 - sz_from(way)

    targets = [depth - 1 - i // 2 if i % 2 == 0 else i // 2 for i in range(depth)]

    def sc_event(t):
        for part in range(PARTS):
            sc_copy(t, part).wait_recv()
            c_buf[t, part] = (
                c_buf[t, part].astype(F32) + gi[g_rows(t, core, part), :].astype(F32)
            ).astype(bf16)

    def sz_start():
        for step in range(depth - 1):
            for part in range(PARTS):
                for way in range(2):

                    @pl.when(sz_from(way) == 0)
                    def _():
                        sz_copy(way, step, part).start()

    def sz_event(hop, part):
        for way in range(2):
            step = hop - sz_from(way)

            @pl.when(jnp.logical_and(sz_from(way) > 0, step >= 0))
            def _():
                sz_copy(way, step, part).wait_recv()

                @pl.when(s_sends(way, step))
                def _():
                    t = sz_target(way, step)
                    c_buf[t, part] = (
                        c_buf[t, part].astype(F32) + z_buf[way, step, part].astype(F32)
                    ).astype(bf16)
                    sz_copy(way, step, part).start()

    def sz_finish():
        zero = jnp.zeros((sub, width), F32)
        for part in range(PARTS):
            total = c_buf[z, part].astype(F32)
            from_left = z_buf[0, jnp.clip(depth - 1 - z, 0, depth - 2), part].astype(F32)
            from_right = z_buf[1, jnp.clip(z, 0, depth - 2), part].astype(F32)
            total += jnp.where(z > 0, from_left, zero)
            total += jnp.where(z < depth - 1, from_right, zero)
            gi_res[pl.ds(part * sub, sub), :] = total.astype(bf16)
        pltpu.make_async_copy(gi_res, outs[0], o_sem.at[0]).start()

    tile = min(256, rows_all)

    def over_tiles(step):
        def run(i, carry):
            step(pl.ds(pl.multiple_of(i * tile, tile), tile))
            return carry

        lax.fori_loop(0, rows_all // tile, run, 0)

    def gate_step(at):
        act_buf[:, at] = nt(gate_full[...], tok_all[at, :])

    def up_step(at):
        up_pre = nt(up_full[...], tok_all[at, :])
        gate_pre = act_buf[:, at]
        sig = jax.nn.sigmoid(gate_pre)
        active = gate_pre * sig
        hid_t[:, at] = (active * up_pre).astype(bf16)
        act_buf[:, at] = active
        fac_buf[:, at] = up_pre * sig * (1.0 + gate_pre * (1.0 - sig))

    def down_step(at):
        d_hidden = nt(down_full[...], cot_all[at, :])
        d_gate = d_hidden * fac_buf[:, at]
        d_up = d_hidden * act_buf[:, at]
        dgate_t[:, at] = d_gate.astype(bf16)
        dup_t[:, at] = d_up.astype(bf16)
        dgate[at, :] = d_gate.T.astype(bf16)
        dup[at, :] = d_up.T.astype(bf16)

    gi_tile = min(512, width)

    def gi_steps(first, last):
        def run(i, carry):
            at = pl.ds(pl.multiple_of(i * gi_tile, gi_tile), gi_tile)
            gi[:, at] = (nn(dgate[...], gate_full[:, at]) + nn(dup[...], up_full[:, at])).astype(bf16)
            return carry

        lax.fori_loop(first, last, run, 0)

    TOK, COT = 0, 1
    GATE, UP, DOWN = 0, 1, 2

    gz_start(TOK)
    gw_start(GATE)
    gz_event(TOK, 0, 0)
    gw_relays(GATE)
    gw_start(UP)
    for part in range(1, PARTS):
        gz_event(TOK, 0, part)
    gz_events(TOK, 1, depth - 2)
    gz_start(COT)
    gw_finish(GATE)
    gz_event(TOK, depth - 2, 0)
    gw_relays(UP)
    gw_start(DOWN)
    for part in range(1, PARTS):
        gz_event(TOK, depth - 2, part)
    gc_finish(TOK)
    over_tiles(gate_step)
    gz_events(COT, 0, 1)
    gw_finish(UP)
    over_tiles(up_step)
    gz_events(COT, 1, depth - 2)
    gw_relays(DOWN)
    gz_events(COT, depth - 2, depth - 1)
    gc_finish(COT)
    weight_grad(2, hid_t, cot_all)
    gw_finish(DOWN)
    over_tiles(down_step)
    gi_count = width // gi_tile
    gi_steps(0, gi_count // 2)
    sw_relay(2)
    gi_steps(gi_count // 2, gi_count)
    for t in targets:
        for part in range(PARTS):
            sc_copy(t, part).start()
    weight_grad(0, dgate_t, tok_all)
    for t in targets:
        sc_event(t)
    sz_start()
    weight_grad(1, dup_t, tok_all)
    sw_finish(2)
    for hop in range(1, depth):
        for part in range(PARTS):
            sz_event(hop, part)
        if hop == 1:
            sw_relay(0)
        if hop == max(depth - 2, 1):
            sw_relay(1)
    sz_finish()
    sw_finish(0)
    sw_finish(1)

    for array in range(2):
        for part in range(PARTS):
            gc_copy(array, 0, -1, part).wait_send()
            for way in range(2):
                for step in range(depth - 1):

                    @pl.when(g_sends(way, step))
                    def _():
                        gz_copy(array, way, step, part).wait_send()

                    @pl.when(g_arrives(way, step))
                    def _():
                        gc_copy(array, way, step, part).wait_send()

    for array in range(3):
        for split in range(2):
            order = orders[split]
            for phase in range(phases):
                for index in range(1 << phase):
                    mask = sum(order[i] for i in range(phase) if index & (1 << i))
                    gw_copy(array, split, phase, mask).wait_send()
            for mask in range(1, n_fs):
                sw_copy(array, split, mask).wait_send()

    for part in range(PARTS):
        for t in targets:
            sc_copy(t, part).wait_send()
        for way in range(2):
            for step in range(depth - 1):

                @pl.when(s_sends(way, step))
                def _():
                    sz_copy(way, step, part).wait_send()

    pltpu.make_async_copy(gi_res, outs[0], o_sem.at[0]).wait()
    for array in range(3):
        pltpu.make_async_copy(w_res[array], outs[1 + array], o_sem.at[1 + array]).wait()


def layer(n_fs, n_tp, tokens, gate, up, down, cot):
    depth = n_tp // CORES
    n, width = tokens.shape
    ff, cols = gate.shape
    rows_all = n * n_tp
    bf16 = tokens.dtype
    hbm = pl.BlockSpec(memory_space=pl.ANY)
    vmem = pltpu.VMEM
    dma = pltpu.SemaphoreType.DMA
    half, sub = ff // 2, n // PARTS
    n_stage = max(n_fs // 2 - 1, 1)
    scratch = (
        [vmem((rows_all, width), bf16)] * 2
        + [vmem((ff, width), bf16)] * 3
        + [vmem((ff, rows_all), F32)] * 2
        + [vmem((ff, rows_all), bf16)] * 3
        + [vmem((rows_all, ff), bf16)] * 2
        + [vmem((ff, width), bf16)] * 3
        + [vmem((2, n_fs - 1, half, cols), bf16)] * 3
        + [vmem((2, n_stage, half, cols), bf16)] * 3
        + [vmem((ff, cols), F32)] * 3
        + [
            vmem((rows_all, width), bf16),
            vmem((depth, PARTS, sub, width), bf16),
            vmem((2, depth - 1, PARTS, sub, width), bf16),
            vmem((n, width), bf16),
        ]
        + [
            dma((3, 2, n_fs - 1)),
            dma((3, 2, n_fs - 1)),
            dma((2, 2, depth - 1, PARTS)),
            dma((2, 2, depth - 1, PARTS)),
            dma((2, 2, depth, PARTS)),
            dma((2, 2, depth, PARTS)),
            dma((5,)),
            dma((3, 2, n_fs - 1)),
            dma((3, 2, n_fs - 1)),
            dma((2, depth - 1, PARTS)),
            dma((2, depth - 1, PARTS)),
            dma((depth, PARTS)),
            dma((depth, PARTS)),
            dma((4,)),
        ]
    )
    return pl.pallas_call(
        functools.partial(layer_kernel, n_fs, n_tp),
        out_shape=(jax.ShapeDtypeStruct((n, width), bf16),)
        + tuple(jax.ShapeDtypeStruct((ff, cols), F32) for _ in range(3)),
        in_specs=[hbm] * 5,
        out_specs=[hbm] * 4,
        scratch_shapes=scratch,
        compiler_params=pltpu.CompilerParams(
            collective_id=0, has_side_effects=True, vmem_limit_bytes=67043328
        ),
        name="layer",
    )(tokens, gate, up, down, cot)


def body(n_fs, n_tp, tokens, gate_weight, up_weight, down_weight, grad_out):
    grad_input, grad_gate, grad_up, grad_down = layer(
        n_fs, n_tp, tokens, gate_weight.T, up_weight.T, down_weight, grad_out
    )
    return grad_input, grad_gate.T, grad_up.T, grad_down


def solution(mesh):
    in_specs = (
        P(("fs", "tp"), None),
        P("fs", "tp"),
        P("fs", "tp"),
        P("tp", "fs"),
        P(("fs", "tp"), None),
    )
    out_specs = (P(("fs", "tp"), None), P("fs", "tp"), P("fs", "tp"), P("tp", "fs"))
    return jax.shard_map(
        functools.partial(body, mesh.shape["fs"], mesh.shape["tp"]),
        mesh=mesh,
        in_specs=in_specs,
        out_specs=out_specs,
        check_vma=False,
    )
```

```python
import functools

import jax
import jax.numpy as jnp
from jax import lax
from jax.experimental import pallas as pl
from jax.experimental.pallas import tpu as pltpu
from jax.sharding import PartitionSpec as P

MESH = pl.DeviceIdType.MESH
CORES = 2
PARTS = 2
F32 = jnp.float32


def nt(left, right):
    return lax.dot_general(left, right, (((1,), (1,)), ((), ())), preferred_element_type=F32)


def nn(left, right):
    return jnp.dot(left, right, preferred_element_type=F32)


def orders_of(n_fs):
    bits = [1 << i for i in range(n_fs.bit_length() - 1)]
    return (bits, bits[::-1])


def first_bit(order, mask):
    return next(i for i, bit in enumerate(order) if mask & bit)


def compact(order, mask):
    return sum(1 << i for i, bit in enumerate(order) if mask & bit)


def greet(n_fs, depth, fs, tp, z):
    barrier = pltpu.get_barrier_semaphore()
    bits = orders_of(n_fs)[0]

    def hello(fs_id, tp_id):
        pl.semaphore_signal(barrier, inc=1, device_id=(fs_id, tp_id), device_id_type=MESH)

    for bit in bits:
        hello(fs ^ bit, tp)
    hello(fs, tp ^ 1)

    @pl.when(z > 0)
    def _():
        hello(fs, tp - CORES)

    @pl.when(z < depth - 1)
    def _():
        hello(fs, tp + CORES)

    ends = (z > 0).astype(jnp.int32) + (z < depth - 1).astype(jnp.int32)
    pl.semaphore_wait(barrier, len(bits) + 1 + ends)


def layer_kernel(n_fs, n_tp, *refs):
    ins, outs, scratch = refs[:5], refs[5:9], refs[9:]
    tok_all, cot_all, gate_full, up_full, down_full = scratch[:5]
    act_buf, fac_buf, hid_t, dgate_t, dup_t, dgate, dup = scratch[5:12]
    grads, recvs, stages = scratch[12:15], scratch[15:18], scratch[18:21]
    gi, c_buf, z_buf = scratch[21:24]
    gw_send, gw_recv, gz_send, gz_recv, gc_send, gc_recv, l_sem = scratch[24:31]
    sw_send, sw_recv, sz_send, sz_recv, sc_send, sc_recv = scratch[31:]
    fs, tp = lax.axis_index("fs"), lax.axis_index("tp")
    depth = n_tp // CORES
    z, core = tp // CORES, tp % CORES
    orders = orders_of(n_fs)
    phases = len(orders[0])
    bf16 = tok_all.dtype
    rows_all, width = tok_all.shape
    n = rows_all // n_tp
    ff = gate_full.shape[0]
    cols = width // n_fs
    half = ff // 2
    sub = n // PARTS
    rows = (tok_all, cot_all)
    weights = (gate_full, up_full, down_full)
    gi_res, *w_res = outs

    def slab(owner):
        return pl.ds(pl.multiple_of(owner * cols, cols), cols)

    def own_rows(owner):
        return pl.ds(pl.multiple_of(owner * n, n), n)

    local = [
        pltpu.make_async_copy(ins[0], tok_all.at[own_rows(tp), :], l_sem.at[0]),
        pltpu.make_async_copy(ins[1], gate_full.at[:, slab(fs)], l_sem.at[1]),
        pltpu.make_async_copy(ins[2], up_full.at[:, slab(fs)], l_sem.at[2]),
        pltpu.make_async_copy(ins[3], down_full.at[:, slab(fs)], l_sem.at[3]),
        pltpu.make_async_copy(ins[4], cot_all.at[own_rows(tp), :], l_sem.at[4]),
    ]
    for copy in local:
        copy.start()
    greet(n_fs, depth, fs, tp, z)
    for copy in local:
        copy.wait()

    def gw_copy(array, split, phase, mask):
        order = orders[split]
        there = weights[array].at[pl.ds(split * half, half), slab(fs ^ mask)]
        slot = (array, split, (1 << phase) - 1 + sum(1 << i for i in range(phase) if mask & order[i]))
        return pltpu.make_async_remote_copy(
            src_ref=there,
            dst_ref=there,
            send_sem=gw_send.at[slot],
            recv_sem=gw_recv.at[slot],
            device_id=(fs ^ order[phase], tp),
            device_id_type=MESH,
        )

    def gw_start(array):
        for phase in range(phases):
            for split in range(2):
                gw_copy(array, split, phase, 0).start()

    def gw_event(array, phase, index):
        for split in range(2):
            order = orders[split]
            mask = sum(order[i] for i in range(phase) if index & (1 << i))
            gw_copy(array, split, phase, mask).wait_recv()
            got = mask | order[phase]
            for later in range(phase + 1, phases):
                gw_copy(array, split, later, got).start()

    def gw_relays(array):
        for phase in range(phases - 1):
            for index in range(1 << phase):
                gw_event(array, phase, index)

    def gw_finish(array):
        for index in range(1 << (phases - 1)):
            gw_event(array, phases - 1, index)

    def r_block(array, owner, part):
        start = pl.multiple_of(owner * n + part * sub, sub)
        return rows[array].at[pl.ds(start, sub), :]

    def gz_copy(array, way, step, part):
        sign = 1 if way == 0 else -1
        there = r_block(array, tp - sign * step * CORES, part)
        slot = (array, way, step, part)
        return pltpu.make_async_remote_copy(
            src_ref=there,
            dst_ref=there,
            send_sem=gz_send.at[slot],
            recv_sem=gz_recv.at[slot],
            device_id=(fs, tp + sign * CORES),
            device_id_type=MESH,
        )

    def g_sends(way, step):
        if way == 0:
            return jnp.logical_and(z - step >= 0, z < depth - 1)
        return jnp.logical_and(z + step <= depth - 1, z > 0)

    def g_arrives(way, step):
        return z - 1 - step >= 0 if way == 0 else z + 1 + step <= depth - 1

    def gc_copy(array, way, step, part):
        sign = 1 if way == 0 else -1
        there = r_block(array, tp - sign * (step + 1) * CORES, part)
        slot = (array, way, step + 1, part)
        return pltpu.make_async_remote_copy(
            src_ref=there,
            dst_ref=there,
            send_sem=gc_send.at[slot],
            recv_sem=gc_recv.at[slot],
            device_id=(fs, tp ^ 1),
            device_id_type=MESH,
        )

    def gz_start(array):
        for part in range(PARTS):
            for way in range(2):

                @pl.when(g_sends(way, 0))
                def _():
                    gz_copy(array, way, 0, part).start()

            gc_copy(array, 0, -1, part).start()

    def gz_event(array, step, part):
        for way in range(2):

            @pl.when(g_arrives(way, step))
            def _():
                gz_copy(array, way, step, part).wait_recv()

            if step + 1 < depth - 1:

                @pl.when(g_sends(way, step + 1))
                def _():
                    gz_copy(array, way, step + 1, part).start()

            @pl.when(g_arrives(way, step))
            def _():
                gc_copy(array, way, step, part).start()

    def gz_events(array, first, last):
        for step in range(first, last):
            for part in range(PARTS):
                gz_event(array, step, part)

    def gc_finish(array):
        for part in range(PARTS):
            gc_copy(array, 0, -1, part).wait_recv()
            for way in range(2):
                for step in range(depth - 1):

                    @pl.when(g_arrives(way, step))
                    def _():
                        gc_copy(array, way, step, part).wait_recv()

    def sw_own(array, split, mask):
        return grads[array].at[pl.ds(split * half, half), slab(fs ^ mask)]

    def sw_copy(array, split, mask):
        order = orders[split]
        phase = first_bit(order, mask)
        slot = compact(order, mask) - 1
        src = sw_own(array, split, mask) if phase == 0 else stages[array].at[split, slot // 2]
        return pltpu.make_async_remote_copy(
            src_ref=src,
            dst_ref=recvs[array].at[split, slot],
            send_sem=sw_send.at[array, split, slot],
            recv_sem=sw_recv.at[array, split, slot],
            device_id=(fs ^ order[phase], tp),
            device_id_type=MESH,
        )

    def sw_sum(array, split, mask):
        order = orders[split]
        total = sw_own(array, split, mask)[...].astype(F32)
        limit = phases if mask == 0 else first_bit(order, mask)
        for phase in range(limit):
            sent = mask | order[phase]
            sw_copy(array, split, sent).wait_recv()
            total += recvs[array][split, compact(order, sent) - 1].astype(F32)
        return total

    later = [m for m in range(1, n_fs) if not m & 1]
    later = sorted(later, key=lambda m: ((m & -m), -m))

    def sw_relay(array):
        for mask in later:
            for split in range(2):
                order = orders[split]
                real = sum(bit for i, bit in enumerate(order) if mask & (1 << i))
                slot = mask - 1
                stages[array][split, slot // 2] = sw_sum(array, split, real).astype(bf16)
                sw_copy(array, split, real).start()

    def sw_finish(array):
        for split in range(2):
            w_res[array][pl.ds(split * half, half), :] = sw_sum(array, split, 0)

    firsts = (orders[0][0], orders[1][0])
    masks = sorted(
        range(n_fs), key=lambda m: (-sum(1 for b in firsts if m & b), -m)
    )

    def weight_grad(array, left, right):
        for mask in masks:
            grads[array][:, slab(fs ^ mask)] = nn(left[...], right[:, slab(fs ^ mask)]).astype(bf16)
            for split in range(2):
                if mask & firsts[split]:
                    sw_copy(array, split, mask).start()

    def g_rows(target, which, part):
        start = (target * CORES + which) * n + part * sub
        return pl.ds(pl.multiple_of(start, sub), sub)

    def sc_copy(target, part):
        return pltpu.make_async_remote_copy(
            src_ref=gi.at[g_rows(target, 1 - core, part), :],
            dst_ref=c_buf.at[target, part],
            send_sem=sc_send.at[target, part],
            recv_sem=sc_recv.at[target, part],
            device_id=(fs, tp ^ 1),
            device_id_type=MESH,
        )

    def sz_from(way):
        return z if way == 0 else depth - 1 - z

    def sz_target(way, step):
        return depth - 1 - step if way == 0 else step

    def sz_copy(way, step, part):
        return pltpu.make_async_remote_copy(
            src_ref=c_buf.at[sz_target(way, step), part],
            dst_ref=z_buf.at[way, step, part],
            send_sem=sz_send.at[way, step, part],
            recv_sem=sz_recv.at[way, step, part],
            device_id=(fs, tp + CORES if way == 0 else tp - CORES),
            device_id_type=MESH,
        )

    def s_sends(way, step):
        return step < depth - 1 - sz_from(way)

    targets = [depth - 1 - i // 2 if i % 2 == 0 else i // 2 for i in range(depth)]

    def sc_event(t):
        for part in range(PARTS):
            sc_copy(t, part).wait_recv()
            c_buf[t, part] = (
                c_buf[t, part].astype(F32) + gi[g_rows(t, core, part), :].astype(F32)
            ).astype(bf16)

    def sz_start():
        for step in range(depth - 1):
            for part in range(PARTS):
                for way in range(2):

                    @pl.when(sz_from(way) == 0)
                    def _():
                        sz_copy(way, step, part).start()

    def sz_event(hop, part):
        for way in range(2):
            step = hop - sz_from(way)

            @pl.when(jnp.logical_and(sz_from(way) > 0, step >= 0))
            def _():
                sz_copy(way, step, part).wait_recv()

                @pl.when(s_sends(way, step))
                def _():
                    t = sz_target(way, step)
                    c_buf[t, part] = (
                        c_buf[t, part].astype(F32) + z_buf[way, step, part].astype(F32)
                    ).astype(bf16)
                    sz_copy(way, step, part).start()

    def sz_finish():
        zero = jnp.zeros((sub, width), F32)
        for part in range(PARTS):
            total = c_buf[z, part].astype(F32)
            from_left = z_buf[0, jnp.clip(depth - 1 - z, 0, depth - 2), part].astype(F32)
            from_right = z_buf[1, jnp.clip(z, 0, depth - 2), part].astype(F32)
            total += jnp.where(z > 0, from_left, zero)
            total += jnp.where(z < depth - 1, from_right, zero)
            gi_res[pl.ds(part * sub, sub), :] = total.astype(bf16)

    def g_drain():
        for array in range(2):
            for part in range(PARTS):
                gc_copy(array, 0, -1, part).wait_send()
                for way in range(2):
                    for step in range(depth - 1):

                        @pl.when(g_sends(way, step))
                        def _():
                            gz_copy(array, way, step, part).wait_send()

                        @pl.when(g_arrives(way, step))
                        def _():
                            gc_copy(array, way, step, part).wait_send()

        for array in range(3):
            for split in range(2):
                order = orders[split]
                for phase in range(phases):
                    for index in range(1 << phase):
                        mask = sum(order[i] for i in range(phase) if index & (1 << i))
                        gw_copy(array, split, phase, mask).wait_send()

    def sz_drain():
        for part in range(PARTS):
            for t in targets:
                sc_copy(t, part).wait_send()
            for way in range(2):
                for step in range(depth - 1):

                    @pl.when(s_sends(way, step))
                    def _():
                        sz_copy(way, step, part).wait_send()

    def sw_drain(array):
        for split in range(2):
            for mask in range(1, n_fs):
                sw_copy(array, split, mask).wait_send()

    tile = min(256, rows_all)

    def over_tiles(step):
        def run(i, carry):
            step(pl.ds(pl.multiple_of(i * tile, tile), tile))
            return carry

        lax.fori_loop(0, rows_all // tile, run, 0)

    def gate_step(at):
        act_buf[:, at] = nt(gate_full[...], tok_all[at, :])

    def up_step(at):
        up_pre = nt(up_full[...], tok_all[at, :])
        gate_pre = act_buf[:, at]
        sig = jax.nn.sigmoid(gate_pre)
        active = gate_pre * sig
        hid_t[:, at] = (active * up_pre).astype(bf16)
        act_buf[:, at] = active
        fac_buf[:, at] = up_pre * sig * (1.0 + gate_pre * (1.0 - sig))

    def down_step(at):
        d_hidden = nt(down_full[...], cot_all[at, :])
        d_gate = d_hidden * fac_buf[:, at]
        d_up = d_hidden * act_buf[:, at]
        dgate_t[:, at] = d_gate.astype(bf16)
        dup_t[:, at] = d_up.astype(bf16)
        dgate[at, :] = d_gate.T.astype(bf16)
        dup[at, :] = d_up.T.astype(bf16)

    gi_tile = min(512, width)

    def gi_steps(first, last):
        def run(i, carry):
            at = pl.ds(pl.multiple_of(i * gi_tile, gi_tile), gi_tile)
            gi[:, at] = (nn(dgate[...], gate_full[:, at]) + nn(dup[...], up_full[:, at])).astype(bf16)
            return carry

        lax.fori_loop(first, last, run, 0)

    TOK, COT = 0, 1
    GATE, UP, DOWN = 0, 1, 2

    gz_start(TOK)
    gw_start(GATE)
    gz_event(TOK, 0, 0)
    gw_relays(GATE)
    gw_start(UP)
    for part in range(1, PARTS):
        gz_event(TOK, 0, part)
    gz_events(TOK, 1, depth - 2)
    gz_start(COT)
    gw_finish(GATE)
    gz_event(TOK, depth - 2, 0)
    gw_relays(UP)
    gw_start(DOWN)
    for part in range(1, PARTS):
        gz_event(TOK, depth - 2, part)
    gc_finish(TOK)
    over_tiles(gate_step)
    gz_events(COT, 0, 1)
    gw_finish(UP)
    over_tiles(up_step)
    gz_events(COT, 1, depth - 2)
    gw_relays(DOWN)
    gz_events(COT, depth - 2, depth - 1)
    gc_finish(COT)
    weight_grad(2, hid_t, cot_all)
    gw_finish(DOWN)
    over_tiles(down_step)
    gi_count = width // gi_tile
    gi_steps(0, gi_count // 2)
    sw_relay(2)
    gi_steps(gi_count // 2, gi_count)
    for t in targets:
        for part in range(PARTS):
            sc_copy(t, part).start()
    weight_grad(0, dgate_t, tok_all)
    for t in targets:
        sc_event(t)
    sz_start()
    weight_grad(1, dup_t, tok_all)
    g_drain()
    sw_finish(2)
    sw_drain(2)
    for hop in range(1, depth):
        for part in range(PARTS):
            sz_event(hop, part)
        if hop == 1:
            sw_relay(0)
        if hop == max(depth - 2, 1):
            sw_relay(1)
    sz_finish()
    sz_drain()
    sw_finish(0)
    sw_finish(1)

    sw_drain(0)
    sw_drain(1)


def layer(n_fs, n_tp, tokens, gate, up, down, cot):
    depth = n_tp // CORES
    n, width = tokens.shape
    ff, cols = gate.shape
    rows_all = n * n_tp
    bf16 = tokens.dtype
    hbm = pl.BlockSpec(memory_space=pl.ANY)
    vmem = pltpu.VMEM
    dma = pltpu.SemaphoreType.DMA
    half, sub = ff // 2, n // PARTS
    n_stage = max(n_fs // 2 - 1, 1)
    scratch = (
        [vmem((rows_all, width), bf16)] * 2
        + [vmem((ff, width), bf16)] * 3
        + [vmem((ff, rows_all), F32)] * 2
        + [vmem((ff, rows_all), bf16)] * 3
        + [vmem((rows_all, ff), bf16)] * 2
        + [vmem((ff, width), bf16)] * 3
        + [vmem((2, n_fs - 1, half, cols), bf16)] * 3
        + [vmem((2, n_stage, half, cols), bf16)] * 3
        + [
            vmem((rows_all, width), bf16),
            vmem((depth, PARTS, sub, width), bf16),
            vmem((2, depth - 1, PARTS, sub, width), bf16),
        ]
        + [
            dma((3, 2, n_fs - 1)),
            dma((3, 2, n_fs - 1)),
            dma((2, 2, depth - 1, PARTS)),
            dma((2, 2, depth - 1, PARTS)),
            dma((2, 2, depth, PARTS)),
            dma((2, 2, depth, PARTS)),
            dma((5,)),
            dma((3, 2, n_fs - 1)),
            dma((3, 2, n_fs - 1)),
            dma((2, depth - 1, PARTS)),
            dma((2, depth - 1, PARTS)),
            dma((depth, PARTS)),
            dma((depth, PARTS)),
        ]
    )
    return pl.pallas_call(
        functools.partial(layer_kernel, n_fs, n_tp),
        out_shape=(vmem((n, width), bf16),) + (vmem((ff, cols), F32),) * 3,
        in_specs=[hbm] * 5,
        out_specs=[pl.BlockSpec(memory_space=vmem)] * 4,
        scratch_shapes=scratch,
        compiler_params=pltpu.CompilerParams(
            collective_id=0, has_side_effects=True, vmem_limit_bytes=61000000
        ),
        name="layer",
    )(tokens, gate, up, down, cot)


def deliver_kernel(*refs):
    ins, outs, sem = refs[:4], refs[4:8], refs[8]
    copies = [pltpu.make_async_copy(a, b, sem.at[i]) for i, (a, b) in enumerate(zip(ins, outs))]
    for copy in copies:
        copy.start()
    for copy in copies:
        copy.wait()


def deliver(*arrays):
    return pl.pallas_call(
        deliver_kernel,
        out_shape=tuple(jax.ShapeDtypeStruct(a.shape, a.dtype) for a in arrays),
        in_specs=[pl.BlockSpec(memory_space=pltpu.VMEM)] * 4,
        out_specs=[pl.BlockSpec(memory_space=pl.ANY)] * 4,
        scratch_shapes=[pltpu.SemaphoreType.DMA((4,))],
        compiler_params=pltpu.CompilerParams(vmem_limit_bytes=1 << 20),
        name="deliver",
    )(*arrays)


def body(n_fs, n_tp, tokens, gate_weight, up_weight, down_weight, grad_out):
    results = layer(n_fs, n_tp, tokens, gate_weight.T, up_weight.T, down_weight, grad_out)
    grad_input, grad_gate, grad_up, grad_down = deliver(*results)
    return grad_input, grad_gate.T, grad_up.T, grad_down


def solution(mesh):
    in_specs = (
        P(("fs", "tp"), None),
        P("fs", "tp"),
        P("fs", "tp"),
        P("tp", "fs"),
        P(("fs", "tp"), None),
    )
    out_specs = (P(("fs", "tp"), None), P("fs", "tp"), P("fs", "tp"), P("tp", "fs"))
    return jax.shard_map(
        functools.partial(body, mesh.shape["fs"], mesh.shape["tp"]),
        mesh=mesh,
        in_specs=in_specs,
        out_specs=out_specs,
        check_vma=False,
    )
```

```python
import functools

import jax
import jax.numpy as jnp
from jax import lax
from jax.experimental import pallas as pl
from jax.experimental.pallas import tpu as pltpu
from jax.sharding import PartitionSpec as P

MESH = pl.DeviceIdType.MESH
CORES = 2
PARTS = 2
F32 = jnp.float32


def nt(left, right):
    return lax.dot_general(left, right, (((1,), (1,)), ((), ())), preferred_element_type=F32)


def nn(left, right):
    return jnp.dot(left, right, preferred_element_type=F32)


def orders_of(n_fs):
    bits = [1 << i for i in range(n_fs.bit_length() - 1)]
    return (bits, bits[::-1])


def first_bit(order, mask):
    return next(i for i, bit in enumerate(order) if mask & bit)


def compact(order, mask):
    return sum(1 << i for i, bit in enumerate(order) if mask & bit)


def wait_bytes(ref, sem):
    pltpu.make_async_copy(ref, ref, sem).wait()


def greet(n_fs, depth, fs, tp, z):
    barrier = pltpu.get_barrier_semaphore()
    bits = orders_of(n_fs)[0]

    def hello(fs_id, tp_id):
        pl.semaphore_signal(barrier, inc=1, device_id=(fs_id, tp_id), device_id_type=MESH)

    for bit in bits:
        hello(fs ^ bit, tp)
    hello(fs, tp ^ 1)

    @pl.when(z > 0)
    def _():
        hello(fs, tp - CORES)

    @pl.when(z < depth - 1)
    def _():
        hello(fs, tp + CORES)

    ends = (z > 0).astype(jnp.int32) + (z < depth - 1).astype(jnp.int32)
    pl.semaphore_wait(barrier, len(bits) + 1 + ends)


def layer_kernel(n_fs, n_tp, *refs):
    ins, outs, scratch = refs[:5], refs[5:9], refs[9:]
    tok_all, cot_all, gate_full, up_full, down_full = scratch[:5]
    act_buf, fac_buf, hid_t, dgate_t, dup_t, dgate, dup = scratch[5:12]
    grads, recvs, stages = scratch[12:15], scratch[15:18], scratch[18:21]
    gi, c_buf, z_buf = scratch[21:24]
    gw_send, gw_recv, gz_send, gz_recv, gc_send, gc_recv, l_sem = scratch[24:31]
    sw_send, sw_recv, sz_send, sz_recv, sc_send, sc_recv = scratch[31:]
    fs, tp = lax.axis_index("fs"), lax.axis_index("tp")
    depth = n_tp // CORES
    z, core = tp // CORES, tp % CORES
    orders = orders_of(n_fs)
    phases = len(orders[0])
    bf16 = tok_all.dtype
    rows_all, width = tok_all.shape
    n = rows_all // n_tp
    ff = gate_full.shape[0]
    cols = width // n_fs
    half = ff // 2
    sub = n // PARTS
    rows = (tok_all, cot_all)
    weights = (gate_full, up_full, down_full)
    gi_res, *w_res = outs

    def slab(owner):
        return pl.ds(pl.multiple_of(owner * cols, cols), cols)

    def own_rows(owner):
        return pl.ds(pl.multiple_of(owner * n, n), n)

    local = [
        pltpu.make_async_copy(ins[0], tok_all.at[own_rows(tp), :], l_sem.at[0]),
        pltpu.make_async_copy(ins[1], gate_full.at[:, slab(fs)], l_sem.at[1]),
        pltpu.make_async_copy(ins[2], up_full.at[:, slab(fs)], l_sem.at[2]),
        pltpu.make_async_copy(ins[3], down_full.at[:, slab(fs)], l_sem.at[3]),
        pltpu.make_async_copy(ins[4], cot_all.at[own_rows(tp), :], l_sem.at[4]),
    ]
    for copy in local:
        copy.start()
    greet(n_fs, depth, fs, tp, z)
    for copy in local:
        copy.wait()

    def gw_copy(array, split, phase, mask):
        order = orders[split]
        there = weights[array].at[pl.ds(split * half, half), slab(fs ^ mask)]
        slot = (1 << phase) - 1 + sum(1 << i for i in range(phase) if mask & order[i])
        return pltpu.make_async_remote_copy(
            src_ref=there,
            dst_ref=there,
            send_sem=gw_send.at[array],
            recv_sem=gw_recv.at[array, split, min(slot, n_fs // 2 - 1)],
            device_id=(fs ^ order[phase], tp),
            device_id_type=MESH,
        )

    def gw_start(array):
        for phase in range(phases):
            for split in range(2):
                gw_copy(array, split, phase, 0).start()

    def gw_event(array, phase, index):
        for split in range(2):
            order = orders[split]
            mask = sum(order[i] for i in range(phase) if index & (1 << i))
            gw_copy(array, split, phase, mask).wait_recv()
            got = mask | order[phase]
            for later in range(phase + 1, phases):
                gw_copy(array, split, later, got).start()

    def gw_relays(array):
        for phase in range(phases - 1):
            for index in range(1 << phase):
                gw_event(array, phase, index)

    def gw_finish(array):
        last = n_fs // 2
        for split in range(2):
            half_rows = pl.ds(split * half, half)
            landed = weights[array].at[half_rows, pl.ds(0, last * cols)]
            wait_bytes(landed, gw_recv.at[array, split, last - 1])

    def r_block(array, owner, part):
        start = pl.multiple_of(owner * n + part * sub, sub)
        return rows[array].at[pl.ds(start, sub), :]

    def gz_copy(array, way, step, part):
        sign = 1 if way == 0 else -1
        there = r_block(array, tp - sign * step * CORES, part)
        return pltpu.make_async_remote_copy(
            src_ref=there,
            dst_ref=there,
            send_sem=gz_send.at[array, way, step],
            recv_sem=gz_recv.at[array, way, step, part],
            device_id=(fs, tp + sign * CORES),
            device_id_type=MESH,
        )

    def g_sends(way, step):
        if way == 0:
            return jnp.logical_and(z - step >= 0, z < depth - 1)
        return jnp.logical_and(z + step <= depth - 1, z > 0)

    def g_arrives(way, step):
        return z - 1 - step >= 0 if way == 0 else z + 1 + step <= depth - 1

    def gc_copy(array, way, step, part):
        sign = 1 if way == 0 else -1
        there = r_block(array, tp - sign * (step + 1) * CORES, part)
        return pltpu.make_async_remote_copy(
            src_ref=there,
            dst_ref=there,
            send_sem=gc_send.at[array],
            recv_sem=gc_recv.at[array],
            device_id=(fs, tp ^ 1),
            device_id_type=MESH,
        )

    def gz_start(array):
        for part in range(PARTS):
            for way in range(2):

                @pl.when(g_sends(way, 0))
                def _():
                    gz_copy(array, way, 0, part).start()

            gc_copy(array, 0, -1, part).start()

    def gz_event(array, step, part):
        for way in range(2):

            @pl.when(g_arrives(way, step))
            def _():
                gz_copy(array, way, step, part).wait_recv()

            if step + 1 < depth - 1:

                @pl.when(g_sends(way, step + 1))
                def _():
                    gz_copy(array, way, step + 1, part).start()

            @pl.when(g_arrives(way, step))
            def _():
                gc_copy(array, way, step, part).start()

    def gz_events(array, first, last):
        for step in range(first, last):
            for part in range(PARTS):
                gz_event(array, step, part)

    def gc_finish(array):
        wait_bytes(rows[array].at[pl.ds(0, rows_all // CORES), :], gc_recv.at[array])

    def sw_own(array, split, mask):
        return grads[array].at[pl.ds(split * half, half), slab(fs ^ mask)]

    def sw_copy(array, split, mask):
        order = orders[split]
        phase = first_bit(order, mask)
        place = compact(order, mask)
        slot, goal = place - 1, place & (place - 1)
        src = sw_own(array, split, mask) if phase == 0 else stages[array].at[split, slot // 2]
        return pltpu.make_async_remote_copy(
            src_ref=src,
            dst_ref=recvs[array].at[split, slot],
            send_sem=sw_send.at[array],
            recv_sem=sw_recv.at[array, split, goal // 2],
            device_id=(fs ^ order[phase], tp),
            device_id_type=MESH,
        )

    def sw_sum(array, split, mask):
        order = orders[split]
        total = sw_own(array, split, mask)[...].astype(F32)
        limit = phases if mask == 0 else first_bit(order, mask)
        got = recvs[array].at[split, pl.ds(0, limit)]
        wait_bytes(got, sw_recv.at[array, split, compact(order, mask) // 2])
        for phase in range(limit):
            sent = mask | order[phase]
            total += recvs[array][split, compact(order, sent) - 1].astype(F32)
        return total

    later = [m for m in range(1, n_fs) if not m & 1]
    later = sorted(later, key=lambda m: ((m & -m), -m))

    def sw_relay(array):
        for mask in later:
            for split in range(2):
                order = orders[split]
                real = sum(bit for i, bit in enumerate(order) if mask & (1 << i))
                slot = mask - 1
                stages[array][split, slot // 2] = sw_sum(array, split, real).astype(bf16)
                sw_copy(array, split, real).start()

    def sw_finish(array):
        for split in range(2):
            w_res[array][pl.ds(split * half, half), :] = sw_sum(array, split, 0)

    firsts = (orders[0][0], orders[1][0])
    masks = sorted(
        range(n_fs), key=lambda m: (-sum(1 for b in firsts if m & b), -m)
    )

    def weight_grad(array, left, right):
        for mask in masks:
            at = slab(fs ^ mask)
            halves = array == 2 and mask == masks[0]
            if not halves:
                grads[array][:, at] = nn(left[...], right[:, at]).astype(bf16)
            for split in range(2):
                if halves:
                    half_rows = pl.ds(split * half, half)
                    grads[array][half_rows, at] = nn(left[half_rows, :], right[:, at]).astype(bf16)
                if mask & firsts[split]:
                    sw_copy(array, split, mask).start()

    def g_rows(target, which, part):
        start = (target * CORES + which) * n + part * sub
        return pl.ds(pl.multiple_of(start, sub), sub)

    def sc_copy(target, part):
        return pltpu.make_async_remote_copy(
            src_ref=gi.at[g_rows(target, 1 - core, part), :],
            dst_ref=c_buf.at[target, part],
            send_sem=sc_send.at[0],
            recv_sem=sc_recv.at[0],
            device_id=(fs, tp ^ 1),
            device_id_type=MESH,
        )

    def sz_from(way):
        return z if way == 0 else depth - 1 - z

    def sz_target(way, step):
        return depth - 1 - step if way == 0 else step

    def sz_copy(way, step, part):
        return pltpu.make_async_remote_copy(
            src_ref=c_buf.at[sz_target(way, step), part],
            dst_ref=z_buf.at[way, step, part],
            send_sem=sz_send.at[way, step],
            recv_sem=sz_recv.at[way, step, part],
            device_id=(fs, tp + CORES if way == 0 else tp - CORES),
            device_id_type=MESH,
        )

    def s_sends(way, step):
        return step < depth - 1 - sz_from(way)

    targets = [depth - 1 - i // 2 if i % 2 == 0 else i // 2 for i in range(depth)]

    def sc_event(t):
        for part in range(PARTS):
            c_buf[t, part] = (
                c_buf[t, part].astype(F32) + gi[g_rows(t, core, part), :].astype(F32)
            ).astype(bf16)

    def sz_start():
        for step in range(depth - 1):
            for part in range(PARTS):
                for way in range(2):

                    @pl.when(sz_from(way) == 0)
                    def _():
                        sz_copy(way, step, part).start()

    def sz_event(hop, part):
        for way in range(2):
            step = hop - sz_from(way)

            @pl.when(jnp.logical_and(sz_from(way) > 0, step >= 0))
            def _():
                sz_copy(way, step, part).wait_recv()

                @pl.when(s_sends(way, step))
                def _():
                    t = sz_target(way, step)
                    c_buf[t, part] = (
                        c_buf[t, part].astype(F32) + z_buf[way, step, part].astype(F32)
                    ).astype(bf16)
                    sz_copy(way, step, part).start()

    def sz_finish():
        zero = jnp.zeros((sub, width), F32)
        for part in range(PARTS):
            total = c_buf[z, part].astype(F32)
            from_left = z_buf[0, jnp.clip(depth - 1 - z, 0, depth - 2), part].astype(F32)
            from_right = z_buf[1, jnp.clip(z, 0, depth - 2), part].astype(F32)
            total += jnp.where(z > 0, from_left, zero)
            total += jnp.where(z < depth - 1, from_right, zero)
            gi_res[pl.ds(part * sub, sub), :] = total.astype(bf16)

    def g_drain():
        for array in range(2):
            wait_bytes(rows[array].at[pl.ds(0, rows_all // CORES), :], gc_send.at[array])
            for way in range(2):
                for step in range(depth - 1):

                    @pl.when(g_sends(way, step))
                    def _():
                        wait_bytes(rows[array].at[pl.ds(0, n), :], gz_send.at[array, way, step])

        for array in range(3):
            sent = weights[array].at[:, pl.ds(0, (n_fs - 1) * cols)]
            wait_bytes(sent, gw_send.at[array])

    def sz_drain():
        wait_bytes(c_buf, sc_send.at[0])
        for way in range(2):
            for step in range(depth - 1):

                @pl.when(s_sends(way, step))
                def _():
                    wait_bytes(z_buf.at[way, step], sz_send.at[way, step])

    def sw_drain(array):
        sent = grads[array].at[:, pl.ds(0, (n_fs - 1) * cols)]
        wait_bytes(sent, sw_send.at[array])

    tile = min(256, rows_all)

    def over_tiles(step):
        def run(i, carry):
            step(pl.ds(pl.multiple_of(i * tile, tile), tile))
            return carry

        lax.fori_loop(0, rows_all // tile, run, 0)

    def gate_step(at):
        act_buf[:, at] = nt(gate_full[...], tok_all[at, :])

    def up_step(at):
        up_pre = nt(up_full[...], tok_all[at, :])
        gate_pre = act_buf[:, at]
        sig = 1.0 / (1.0 + jnp.exp(-gate_pre))
        active = gate_pre * sig
        hid_t[:, at] = (active * up_pre).astype(bf16)
        act_buf[:, at] = active
        fac_buf[:, at] = up_pre * sig * (1.0 + gate_pre * (1.0 - sig))

    def down_step(at):
        d_hidden = nt(down_full[...], cot_all[at, :])
        d_gate = d_hidden * fac_buf[:, at]
        d_up = d_hidden * act_buf[:, at]
        dgate_t[:, at] = d_gate.astype(bf16)
        dup_t[:, at] = d_up.astype(bf16)
        dgate[at, :] = d_gate.T.astype(bf16)
        dup[at, :] = d_up.T.astype(bf16)

    gi_tile = min(512, width)

    def gi_steps(first, last):
        def run(i, carry):
            at = pl.ds(pl.multiple_of(i * gi_tile, gi_tile), gi_tile)
            gi[:, at] = (nn(dgate[...], gate_full[:, at]) + nn(dup[...], up_full[:, at])).astype(bf16)
            return carry

        lax.fori_loop(first, last, run, 0)

    TOK, COT = 0, 1
    GATE, UP, DOWN = 0, 1, 2

    gz_start(TOK)
    gw_start(GATE)
    gz_event(TOK, 0, 0)
    gw_relays(GATE)
    gw_start(UP)
    for part in range(1, PARTS):
        gz_event(TOK, 0, part)
    gz_events(TOK, 1, depth - 2)
    gz_start(COT)
    gw_finish(GATE)
    gz_event(TOK, depth - 2, 0)
    gw_relays(UP)
    gw_start(DOWN)
    for part in range(1, PARTS):
        gz_event(TOK, depth - 2, part)
    gc_finish(TOK)
    over_tiles(gate_step)
    gz_events(COT, 0, 1)
    gw_finish(UP)
    over_tiles(up_step)
    gz_events(COT, 1, depth - 2)
    gw_relays(DOWN)
    gz_events(COT, depth - 2, depth - 1)
    gc_finish(COT)
    weight_grad(2, hid_t, cot_all)
    gw_finish(DOWN)
    over_tiles(down_step)
    gi_count = width // gi_tile
    gi_steps(0, gi_count // 2)
    sw_relay(2)
    gi_steps(gi_count // 2, gi_count)
    for t in targets:
        for part in range(PARTS):
            sc_copy(t, part).start()
    weight_grad(0, dgate_t, tok_all)
    wait_bytes(c_buf, sc_recv.at[0])
    for t in targets:
        sc_event(t)
    sz_start()
    weight_grad(1, dup_t, tok_all)
    g_drain()
    sw_finish(2)
    sw_drain(2)
    for hop in range(1, depth):
        for part in range(PARTS):
            sz_event(hop, part)
        if hop == 1:
            sw_relay(0)
        if hop == max(depth - 2, 1):
            sw_relay(1)
    sz_finish()
    sz_drain()
    sw_finish(0)
    sw_finish(1)

    sw_drain(0)
    sw_drain(1)


def layer(n_fs, n_tp, tokens, gate, up, down, cot):
    depth = n_tp // CORES
    n, width = tokens.shape
    ff, cols = gate.shape
    rows_all = n * n_tp
    bf16 = tokens.dtype
    hbm = pl.BlockSpec(memory_space=pl.ANY)
    vmem = pltpu.VMEM
    dma = pltpu.SemaphoreType.DMA
    half, sub = ff // 2, n // PARTS
    n_stage = max(n_fs // 2 - 1, 1)
    scratch = (
        [vmem((rows_all, width), bf16)] * 2
        + [vmem((ff, width), bf16)] * 3
        + [vmem((ff, rows_all), F32)] * 2
        + [vmem((ff, rows_all), bf16)] * 3
        + [vmem((rows_all, ff), bf16)] * 2
        + [vmem((ff, width), bf16)] * 3
        + [vmem((2, n_fs - 1, half, cols), bf16)] * 3
        + [vmem((2, n_stage, half, cols), bf16)] * 3
        + [
            vmem((rows_all, width), bf16),
            vmem((depth, PARTS, sub, width), bf16),
            vmem((2, depth - 1, PARTS, sub, width), bf16),
        ]
        + [
            dma((3,)),
            dma((3, 2, n_fs // 2)),
            dma((2, 2, depth - 1)),
            dma((2, 2, depth - 1, PARTS)),
            dma((2,)),
            dma((2,)),
            dma((5,)),
            dma((3,)),
            dma((3, 2, n_fs // 2)),
            dma((2, depth - 1)),
            dma((2, depth - 1, PARTS)),
            dma((1,)),
            dma((1,)),
        ]
    )
    return pl.pallas_call(
        functools.partial(layer_kernel, n_fs, n_tp),
        out_shape=(vmem((n, width), bf16),) + (vmem((ff, cols), F32),) * 3,
        in_specs=[hbm] * 5,
        out_specs=[pl.BlockSpec(memory_space=vmem)] * 4,
        scratch_shapes=scratch,
        compiler_params=pltpu.CompilerParams(
            collective_id=0, has_side_effects=True, vmem_limit_bytes=61000000
        ),
        name="layer",
    )(tokens, gate, up, down, cot)


def deliver_kernel(*refs):
    ins, outs, sem = refs[:4], refs[4:8], refs[8]
    copies = [pltpu.make_async_copy(a, b, sem.at[i]) for i, (a, b) in enumerate(zip(ins, outs))]
    for copy in copies:
        copy.start()
    for copy in copies:
        copy.wait()


def deliver(*arrays):
    return pl.pallas_call(
        deliver_kernel,
        out_shape=tuple(jax.ShapeDtypeStruct(a.shape, a.dtype) for a in arrays),
        in_specs=[pl.BlockSpec(memory_space=pltpu.VMEM)] * 4,
        out_specs=[pl.BlockSpec(memory_space=pl.ANY)] * 4,
        scratch_shapes=[pltpu.SemaphoreType.DMA((4,))],
        compiler_params=pltpu.CompilerParams(vmem_limit_bytes=1 << 20),
        name="deliver",
    )(*arrays)


def body(n_fs, n_tp, tokens, gate_weight, up_weight, down_weight, grad_out):
    results = layer(n_fs, n_tp, tokens, gate_weight.T, up_weight.T, down_weight, grad_out)
    grad_input, grad_gate, grad_up, grad_down = deliver(*results)
    return grad_input, grad_gate.T, grad_up.T, grad_down


def solution(mesh):
    in_specs = (
        P(("fs", "tp"), None),
        P("fs", "tp"),
        P("fs", "tp"),
        P("tp", "fs"),
        P(("fs", "tp"), None),
    )
    out_specs = (P(("fs", "tp"), None), P("fs", "tp"), P("fs", "tp"), P("tp", "fs"))
    return jax.shard_map(
        functools.partial(body, mesh.shape["fs"], mesh.shape["tp"]),
        mesh=mesh,
        in_specs=in_specs,
        out_specs=out_specs,
        check_vma=False,
    )
```

```python
import functools

import jax
import jax.numpy as jnp
from jax import lax
from jax.experimental import pallas as pl
from jax.experimental.pallas import tpu as pltpu
from jax.sharding import PartitionSpec as P

MESH = pl.DeviceIdType.MESH
CORES = 2
PARTS = 2
F32 = jnp.float32


def nt(left, right):
    return lax.dot_general(left, right, (((1,), (1,)), ((), ())), preferred_element_type=F32)


def nn(left, right):
    return jnp.dot(left, right, preferred_element_type=F32)


def orders_of(n_fs):
    bits = [1 << i for i in range(n_fs.bit_length() - 1)]
    return (bits, bits[::-1])


def first_bit(order, mask):
    return next(i for i, bit in enumerate(order) if mask & bit)


def compact(order, mask):
    return sum(1 << i for i, bit in enumerate(order) if mask & bit)


def wait_bytes(ref, sem):
    pltpu.make_async_copy(ref, ref, sem).wait()


def greet(n_fs, depth, fs, tp, z):
    barrier = pltpu.get_barrier_semaphore()
    bits = orders_of(n_fs)[0]

    def hello(fs_id, tp_id):
        pl.semaphore_signal(barrier, inc=1, device_id=(fs_id, tp_id), device_id_type=MESH)

    for bit in bits:
        hello(fs ^ bit, tp)
    hello(fs, tp ^ 1)

    @pl.when(z > 0)
    def _():
        hello(fs, tp - CORES)

    @pl.when(z < depth - 1)
    def _():
        hello(fs, tp + CORES)

    ends = (z > 0).astype(jnp.int32) + (z < depth - 1).astype(jnp.int32)
    pl.semaphore_wait(barrier, len(bits) + 1 + ends)


def layer_kernel(n_fs, n_tp, *refs):
    ins, outs, scratch = refs[:5], refs[5:9], refs[9:]
    tok_all, cot_all, gate_full, up_full, down_full = scratch[:5]
    act_buf, fac_buf, hid_t, dgate_t, dup_t, dgate, dup = scratch[5:12]
    grads, recvs, stages = scratch[12:15], scratch[15:18], scratch[18:21]
    gi, c_buf, z_buf = scratch[21:24]
    gw_send, gw_recv, gz_send, gz_recv, gc_send, gc_recv, l_sem = scratch[24:31]
    sw_send, sw_recv, sz_send, sz_recv, sc_send, sc_recv = scratch[31:]
    fs, tp = lax.axis_index("fs"), lax.axis_index("tp")
    depth = n_tp // CORES
    z, core = tp // CORES, tp % CORES
    orders = orders_of(n_fs)
    phases = len(orders[0])
    bf16 = tok_all.dtype
    rows_all, width = tok_all.shape
    n = rows_all // n_tp
    ff = gate_full.shape[0]
    cols = width // n_fs
    half = ff // 2
    sub = n // PARTS
    rows = (tok_all, cot_all)
    weights = (gate_full, up_full, down_full)
    gi_res, *w_res = outs

    def slab(owner):
        return pl.ds(pl.multiple_of(owner * cols, cols), cols)

    def own_rows(owner):
        return pl.ds(pl.multiple_of(owner * n, n), n)

    local = [
        pltpu.make_async_copy(ins[0], tok_all.at[own_rows(tp), :], l_sem.at[0]),
        pltpu.make_async_copy(ins[1], gate_full.at[:, slab(fs)], l_sem.at[1]),
        pltpu.make_async_copy(ins[2], up_full.at[:, slab(fs)], l_sem.at[2]),
        pltpu.make_async_copy(ins[3], down_full.at[:, slab(fs)], l_sem.at[3]),
        pltpu.make_async_copy(ins[4], cot_all.at[own_rows(tp), :], l_sem.at[4]),
    ]
    for copy in local:
        copy.start()
    greet(n_fs, depth, fs, tp, z)
    for copy in local[:2]:
        copy.wait()

    def gw_copy(array, split, phase, mask):
        order = orders[split]
        there = weights[array].at[pl.ds(split * half, half), slab(fs ^ mask)]
        slot = (1 << phase) - 1 + sum(1 << i for i in range(phase) if mask & order[i])
        return pltpu.make_async_remote_copy(
            src_ref=there,
            dst_ref=there,
            send_sem=gw_send.at[array],
            recv_sem=gw_recv.at[array, split, min(slot, n_fs // 2 - 1)],
            device_id=(fs ^ order[phase], tp),
            device_id_type=MESH,
        )

    def gw_start(array):
        for phase in range(phases):
            for split in range(2):
                gw_copy(array, split, phase, 0).start()

    def gw_event(array, phase, index):
        for split in range(2):
            order = orders[split]
            mask = sum(order[i] for i in range(phase) if index & (1 << i))
            gw_copy(array, split, phase, mask).wait_recv()
            got = mask | order[phase]
            for later in range(phase + 1, phases):
                gw_copy(array, split, later, got).start()

    def gw_relays(array):
        for phase in range(phases - 1):
            for index in range(1 << phase):
                gw_event(array, phase, index)

    def gw_finish(array):
        last = n_fs // 2
        for split in range(2):
            half_rows = pl.ds(split * half, half)
            landed = weights[array].at[half_rows, pl.ds(0, last * cols)]
            wait_bytes(landed, gw_recv.at[array, split, last - 1])

    def r_block(array, owner, part):
        start = pl.multiple_of(owner * n + part * sub, sub)
        return rows[array].at[pl.ds(start, sub), :]

    def gz_copy(array, way, step, part):
        sign = 1 if way == 0 else -1
        there = r_block(array, tp - sign * step * CORES, part)
        return pltpu.make_async_remote_copy(
            src_ref=there,
            dst_ref=there,
            send_sem=gz_send.at[array, way, step],
            recv_sem=gz_recv.at[array, way, step, part],
            device_id=(fs, tp + sign * CORES),
            device_id_type=MESH,
        )

    def g_sends(way, step):
        if way == 0:
            return jnp.logical_and(z - step >= 0, z < depth - 1)
        return jnp.logical_and(z + step <= depth - 1, z > 0)

    def g_arrives(way, step):
        return z - 1 - step >= 0 if way == 0 else z + 1 + step <= depth - 1

    def gc_copy(array, way, step, part):
        sign = 1 if way == 0 else -1
        there = r_block(array, tp - sign * (step + 1) * CORES, part)
        return pltpu.make_async_remote_copy(
            src_ref=there,
            dst_ref=there,
            send_sem=gc_send.at[array],
            recv_sem=gc_recv.at[array],
            device_id=(fs, tp ^ 1),
            device_id_type=MESH,
        )

    def gz_start(array):
        for part in range(PARTS):
            for way in range(2):

                @pl.when(g_sends(way, 0))
                def _():
                    gz_copy(array, way, 0, part).start()

            gc_copy(array, 0, -1, part).start()

    def gz_event(array, step, part):
        for way in range(2):

            @pl.when(g_arrives(way, step))
            def _():
                gz_copy(array, way, step, part).wait_recv()

            if step + 1 < depth - 1:

                @pl.when(g_sends(way, step + 1))
                def _():
                    gz_copy(array, way, step + 1, part).start()

            @pl.when(g_arrives(way, step))
            def _():
                gc_copy(array, way, step, part).start()

    def gz_events(array, first, last):
        for step in range(first, last):
            for part in range(PARTS):
                gz_event(array, step, part)

    def gc_finish(array):
        wait_bytes(rows[array].at[pl.ds(0, rows_all // CORES), :], gc_recv.at[array])

    def sw_own(array, split, mask):
        return grads[array].at[pl.ds(split * half, half), slab(fs ^ mask)]

    def sw_copy(array, split, mask):
        order = orders[split]
        phase = first_bit(order, mask)
        place = compact(order, mask)
        slot, goal = place - 1, place & (place - 1)
        src = sw_own(array, split, mask) if phase == 0 else stages[array].at[split, slot // 2]
        return pltpu.make_async_remote_copy(
            src_ref=src,
            dst_ref=recvs[array].at[split, slot],
            send_sem=sw_send.at[array],
            recv_sem=sw_recv.at[array, split, goal // 2],
            device_id=(fs ^ order[phase], tp),
            device_id_type=MESH,
        )

    def sw_sum(array, split, mask):
        order = orders[split]
        total = sw_own(array, split, mask)[...].astype(F32)
        limit = phases if mask == 0 else first_bit(order, mask)
        got = recvs[array].at[split, pl.ds(0, limit)]
        wait_bytes(got, sw_recv.at[array, split, compact(order, mask) // 2])
        for phase in range(limit):
            sent = mask | order[phase]
            total += recvs[array][split, compact(order, sent) - 1].astype(F32)
        return total

    later = [m for m in range(1, n_fs) if not m & 1]
    later = sorted(later, key=lambda m: ((m & -m), -m))

    def sw_relay(array):
        for mask in later:
            for split in range(2):
                order = orders[split]
                real = sum(bit for i, bit in enumerate(order) if mask & (1 << i))
                slot = mask - 1
                stages[array][split, slot // 2] = sw_sum(array, split, real).astype(bf16)
                sw_copy(array, split, real).start()

    def sw_finish(array):
        for split in range(2):
            w_res[array][pl.ds(split * half, half), :] = sw_sum(array, split, 0)

    firsts = (orders[0][0], orders[1][0])
    masks = sorted(
        range(n_fs), key=lambda m: (-sum(1 for b in firsts if m & b), -m)
    )

    def weight_grad(array, left, right):
        for mask in masks:
            at = slab(fs ^ mask)
            halves = array == 2 and mask == masks[0]
            if not halves:
                grads[array][:, at] = nn(left[...], right[:, at]).astype(bf16)
            for split in range(2):
                if halves:
                    half_rows = pl.ds(split * half, half)
                    grads[array][half_rows, at] = nn(left[half_rows, :], right[:, at]).astype(bf16)
                if mask & firsts[split]:
                    sw_copy(array, split, mask).start()

    def g_rows(target, which, part):
        start = (target * CORES + which) * n + part * sub
        return pl.ds(pl.multiple_of(start, sub), sub)

    def sc_copy(target, part):
        return pltpu.make_async_remote_copy(
            src_ref=gi.at[g_rows(target, 1 - core, part), :],
            dst_ref=c_buf.at[target, part],
            send_sem=sc_send.at[0],
            recv_sem=sc_recv.at[0],
            device_id=(fs, tp ^ 1),
            device_id_type=MESH,
        )

    def sz_from(way):
        return z if way == 0 else depth - 1 - z

    def sz_target(way, step):
        return depth - 1 - step if way == 0 else step

    def sz_copy(way, step, part):
        return pltpu.make_async_remote_copy(
            src_ref=c_buf.at[sz_target(way, step), part],
            dst_ref=z_buf.at[way, step, part],
            send_sem=sz_send.at[way, step],
            recv_sem=sz_recv.at[way, step, part],
            device_id=(fs, tp + CORES if way == 0 else tp - CORES),
            device_id_type=MESH,
        )

    def s_sends(way, step):
        return step < depth - 1 - sz_from(way)

    targets = [depth - 1 - i // 2 if i % 2 == 0 else i // 2 for i in range(depth)]

    def sc_event(t):
        for part in range(PARTS):
            c_buf[t, part] = (
                c_buf[t, part].astype(F32) + gi[g_rows(t, core, part), :].astype(F32)
            ).astype(bf16)

    def sz_start():
        for step in range(depth - 1):
            for part in range(PARTS):
                for way in range(2):

                    @pl.when(sz_from(way) == 0)
                    def _():
                        sz_copy(way, step, part).start()

    def sz_event(hop, part):
        for way in range(2):
            step = hop - sz_from(way)

            @pl.when(jnp.logical_and(sz_from(way) > 0, step >= 0))
            def _():
                sz_copy(way, step, part).wait_recv()

                @pl.when(s_sends(way, step))
                def _():
                    t = sz_target(way, step)
                    c_buf[t, part] = (
                        c_buf[t, part].astype(F32) + z_buf[way, step, part].astype(F32)
                    ).astype(bf16)
                    sz_copy(way, step, part).start()

    def sz_finish():
        zero = jnp.zeros((sub, width), F32)
        for part in range(PARTS):
            total = c_buf[z, part].astype(F32)
            from_left = z_buf[0, jnp.clip(depth - 1 - z, 0, depth - 2), part].astype(F32)
            from_right = z_buf[1, jnp.clip(z, 0, depth - 2), part].astype(F32)
            total += jnp.where(z > 0, from_left, zero)
            total += jnp.where(z < depth - 1, from_right, zero)
            gi_res[pl.ds(part * sub, sub), :] = total.astype(bf16)

    def g_drain():
        for array in range(2):
            wait_bytes(rows[array].at[pl.ds(0, rows_all // CORES), :], gc_send.at[array])
            for way in range(2):
                for step in range(depth - 1):

                    @pl.when(g_sends(way, step))
                    def _():
                        wait_bytes(rows[array].at[pl.ds(0, n), :], gz_send.at[array, way, step])

        for array in range(3):
            sent = weights[array].at[:, pl.ds(0, (n_fs - 1) * cols)]
            wait_bytes(sent, gw_send.at[array])

    def sz_drain():
        wait_bytes(c_buf, sc_send.at[0])
        for way in range(2):
            for step in range(depth - 1):

                @pl.when(s_sends(way, step))
                def _():
                    wait_bytes(z_buf.at[way, step], sz_send.at[way, step])

    def sw_drain(array):
        sent = grads[array].at[:, pl.ds(0, (n_fs - 1) * cols)]
        wait_bytes(sent, sw_send.at[array])

    tile = min(256, rows_all)

    def over_tiles(step):
        def run(i, carry):
            step(pl.ds(pl.multiple_of(i * tile, tile), tile))
            return carry

        lax.fori_loop(0, rows_all // tile, run, 0)

    def gate_step(at):
        act_buf[:, at] = nt(gate_full[...], tok_all[at, :])

    def up_step(at):
        up_pre = nt(up_full[...], tok_all[at, :])
        gate_pre = act_buf[:, at]
        sig = 1.0 / (1.0 + jnp.exp(-gate_pre))
        active = gate_pre * sig
        hid_t[:, at] = (active * up_pre).astype(bf16)
        act_buf[:, at] = active
        fac_buf[:, at] = up_pre * sig * (1.0 + gate_pre * (1.0 - sig))

    def down_step(at):
        d_hidden = nt(down_full[...], cot_all[at, :])
        d_gate = d_hidden * fac_buf[:, at]
        d_up = d_hidden * act_buf[:, at]
        dgate_t[:, at] = d_gate.astype(bf16)
        dup_t[:, at] = d_up.astype(bf16)
        dgate[at, :] = d_gate.T.astype(bf16)
        dup[at, :] = d_up.T.astype(bf16)

    gi_tile = min(512, width)

    def gi_steps(first, last):
        def run(i, carry):
            at = pl.ds(pl.multiple_of(i * gi_tile, gi_tile), gi_tile)
            gi[:, at] = (nn(dgate[...], gate_full[:, at]) + nn(dup[...], up_full[:, at])).astype(bf16)
            return carry

        lax.fori_loop(first, last, run, 0)

    TOK, COT = 0, 1
    GATE, UP, DOWN = 0, 1, 2

    gz_start(TOK)
    gw_start(GATE)
    for copy in local[2:]:
        copy.wait()
    gz_event(TOK, 0, 0)
    gw_relays(GATE)
    gw_start(UP)
    for part in range(1, PARTS):
        gz_event(TOK, 0, part)
    gz_events(TOK, 1, depth - 2)
    gz_start(COT)
    gw_finish(GATE)
    gz_event(TOK, depth - 2, 0)
    gw_relays(UP)
    gw_start(DOWN)
    for part in range(1, PARTS):
        gz_event(TOK, depth - 2, part)
    gc_finish(TOK)
    over_tiles(gate_step)
    gz_events(COT, 0, 1)
    gw_finish(UP)
    over_tiles(up_step)
    gz_events(COT, 1, depth - 2)
    gw_relays(DOWN)
    gz_events(COT, depth - 2, depth - 1)
    gc_finish(COT)
    weight_grad(2, hid_t, cot_all)
    gw_finish(DOWN)
    over_tiles(down_step)
    gi_count = width // gi_tile
    gi_steps(0, gi_count // 2)
    sw_relay(2)
    gi_steps(gi_count // 2, gi_count)
    for t in targets:
        for part in range(PARTS):
            sc_copy(t, part).start()
    weight_grad(0, dgate_t, tok_all)
    wait_bytes(c_buf, sc_recv.at[0])
    for t in targets:
        sc_event(t)
    sz_start()
    weight_grad(1, dup_t, tok_all)
    g_drain()
    sw_finish(2)
    sw_drain(2)
    for hop in range(1, depth):
        for part in range(PARTS):
            sz_event(hop, part)
        if hop == 1:
            sw_relay(0)
        if hop == max(depth - 2, 1):
            sw_relay(1)
    sz_finish()
    sz_drain()
    sw_finish(0)
    sw_finish(1)

    sw_drain(0)
    sw_drain(1)


def layer(n_fs, n_tp, tokens, gate, up, down, cot):
    depth = n_tp // CORES
    n, width = tokens.shape
    ff, cols = gate.shape
    rows_all = n * n_tp
    bf16 = tokens.dtype
    hbm = pl.BlockSpec(memory_space=pl.ANY)
    vmem = pltpu.VMEM
    dma = pltpu.SemaphoreType.DMA
    half, sub = ff // 2, n // PARTS
    n_stage = max(n_fs // 2 - 1, 1)
    scratch = (
        [vmem((rows_all, width), bf16)] * 2
        + [vmem((ff, width), bf16)] * 3
        + [vmem((ff, rows_all), F32)] * 2
        + [vmem((ff, rows_all), bf16)] * 3
        + [vmem((rows_all, ff), bf16)] * 2
        + [vmem((ff, width), bf16)] * 3
        + [vmem((2, n_fs - 1, half, cols), bf16)] * 3
        + [vmem((2, n_stage, half, cols), bf16)] * 3
        + [
            vmem((rows_all, width), bf16),
            vmem((depth, PARTS, sub, width), bf16),
            vmem((2, depth - 1, PARTS, sub, width), bf16),
        ]
        + [
            dma((3,)),
            dma((3, 2, n_fs // 2)),
            dma((2, 2, depth - 1)),
            dma((2, 2, depth - 1, PARTS)),
            dma((2,)),
            dma((2,)),
            dma((5,)),
            dma((3,)),
            dma((3, 2, n_fs // 2)),
            dma((2, depth - 1)),
            dma((2, depth - 1, PARTS)),
            dma((1,)),
            dma((1,)),
        ]
    )
    return pl.pallas_call(
        functools.partial(layer_kernel, n_fs, n_tp),
        out_shape=(vmem((n, width), bf16),) + (vmem((ff, cols), F32),) * 3,
        in_specs=[hbm] * 5,
        out_specs=[pl.BlockSpec(memory_space=vmem)] * 4,
        scratch_shapes=scratch,
        compiler_params=pltpu.CompilerParams(
            collective_id=0, has_side_effects=True, vmem_limit_bytes=61000000
        ),
        name="layer",
    )(tokens, gate, up, down, cot)


def deliver_kernel(*refs):
    ins, outs, sem = refs[:4], refs[4:8], refs[8]
    copies = [pltpu.make_async_copy(a, b, sem.at[i]) for i, (a, b) in enumerate(zip(ins, outs))]
    for copy in copies:
        copy.start()
    for copy in copies:
        copy.wait()


def deliver(*arrays):
    return pl.pallas_call(
        deliver_kernel,
        out_shape=tuple(jax.ShapeDtypeStruct(a.shape, a.dtype) for a in arrays),
        in_specs=[pl.BlockSpec(memory_space=pltpu.VMEM)] * 4,
        out_specs=[pl.BlockSpec(memory_space=pl.ANY)] * 4,
        scratch_shapes=[pltpu.SemaphoreType.DMA((4,))],
        compiler_params=pltpu.CompilerParams(vmem_limit_bytes=1 << 20),
        name="deliver",
    )(*arrays)


def body(n_fs, n_tp, tokens, gate_weight, up_weight, down_weight, grad_out):
    results = layer(n_fs, n_tp, tokens, gate_weight.T, up_weight.T, down_weight, grad_out)
    grad_input, grad_gate, grad_up, grad_down = deliver(*results)
    return grad_input, grad_gate.T, grad_up.T, grad_down


def solution(mesh):
    in_specs = (
        P(("fs", "tp"), None),
        P("fs", "tp"),
        P("fs", "tp"),
        P("tp", "fs"),
        P(("fs", "tp"), None),
    )
    out_specs = (P(("fs", "tp"), None), P("fs", "tp"), P("fs", "tp"), P("tp", "fs"))
    return jax.shard_map(
        functools.partial(body, mesh.shape["fs"], mesh.shape["tp"]),
        mesh=mesh,
        in_specs=in_specs,
        out_specs=out_specs,
        check_vma=False,
    )
```

```python
import functools

import jax
import jax.numpy as jnp
from jax import lax
from jax.experimental import pallas as pl
from jax.experimental.pallas import tpu as pltpu
from jax.sharding import PartitionSpec as P

MESH = pl.DeviceIdType.MESH
CORES = 2
PARTS = 2
F32 = jnp.float32


def nt(left, right):
    return lax.dot_general(left, right, (((1,), (1,)), ((), ())), preferred_element_type=F32)


def nn(left, right):
    return jnp.dot(left, right, preferred_element_type=F32)


def orders_of(n_fs):
    bits = [1 << i for i in range(n_fs.bit_length() - 1)]
    return (bits, bits[::-1])


def first_bit(order, mask):
    return next(i for i, bit in enumerate(order) if mask & bit)


def compact(order, mask):
    return sum(1 << i for i, bit in enumerate(order) if mask & bit)


def wait_bytes(ref, sem):
    pltpu.make_async_copy(ref, ref, sem).wait()


def greet(n_fs, depth, fs, tp, z):
    barrier = pltpu.get_barrier_semaphore()
    bits = orders_of(n_fs)[0]

    def hello(fs_id, tp_id):
        pl.semaphore_signal(barrier, inc=1, device_id=(fs_id, tp_id), device_id_type=MESH)

    for bit in bits:
        hello(fs ^ bit, tp)
    hello(fs, tp ^ 1)

    @pl.when(z > 0)
    def _():
        hello(fs, tp - CORES)

    @pl.when(z < depth - 1)
    def _():
        hello(fs, tp + CORES)

    ends = (z > 0).astype(jnp.int32) + (z < depth - 1).astype(jnp.int32)
    pl.semaphore_wait(barrier, len(bits) + 1 + ends)


def layer_kernel(n_fs, n_tp, *refs):
    ins, outs, scratch = refs[:5], refs[5:9], refs[9:]
    tok_all, cot_all, gate_full, up_full, down_full = scratch[:5]
    act_buf, fac_buf, hid_t, dgate_t, dup_t, dgate, dup = scratch[5:12]
    grads, recvs, stages = scratch[12:15], scratch[15:18], scratch[18:21]
    gi, c_buf, z_buf = scratch[21:24]
    gw_send, gw_recv, gz_send, gz_recv, gc_send, gc_recv, l_sem = scratch[24:31]
    sw_send, sw_recv, sz_send, sz_recv, sc_send, sc_recv = scratch[31:]
    fs, tp = lax.axis_index("fs"), lax.axis_index("tp")
    depth = n_tp // CORES
    z, core = tp // CORES, tp % CORES
    orders = orders_of(n_fs)
    phases = len(orders[0])
    bf16 = tok_all.dtype
    rows_all, width = tok_all.shape
    n = rows_all // n_tp
    ff = gate_full.shape[0]
    cols = width // n_fs
    half = ff // 2
    sub = n // PARTS
    rows = (tok_all, cot_all)
    weights = (gate_full, up_full, down_full)
    gi_res, *w_res = outs

    def slab(owner):
        return pl.ds(pl.multiple_of(owner * cols, cols), cols)

    def own_rows(owner):
        return pl.ds(pl.multiple_of(owner * n, n), n)

    local = [
        pltpu.make_async_copy(ins[0], tok_all.at[own_rows(tp), :], l_sem.at[0]),
        pltpu.make_async_copy(ins[1], gate_full.at[:, slab(fs)], l_sem.at[1]),
        pltpu.make_async_copy(ins[2], up_full.at[:, slab(fs)], l_sem.at[2]),
        pltpu.make_async_copy(ins[3], down_full.at[:, slab(fs)], l_sem.at[2]),
        pltpu.make_async_copy(ins[4], cot_all.at[own_rows(tp), :], l_sem.at[3]),
    ]
    for copy in local:
        copy.start()
    greet(n_fs, depth, fs, tp, z)
    for copy in local[:2]:
        copy.wait()

    def gw_copy(array, split, phase, mask):
        order = orders[split]
        there = weights[array].at[pl.ds(split * half, half), slab(fs ^ mask)]
        slot = (1 << phase) - 1 + sum(1 << i for i in range(phase) if mask & order[i])
        return pltpu.make_async_remote_copy(
            src_ref=there,
            dst_ref=there,
            send_sem=gw_send.at[array],
            recv_sem=gw_recv.at[array, min(slot, n_fs // 2 - 1)],
            device_id=(fs ^ order[phase], tp),
            device_id_type=MESH,
        )

    def gw_start(array):
        for phase in range(phases):
            for split in range(2):
                gw_copy(array, split, phase, 0).start()

    def gw_event(array, phase, index):
        slot = (1 << phase) - 1 + index
        wait_bytes(weights[array].at[:, pl.ds(0, cols)], gw_recv.at[array, slot])
        for split in range(2):
            order = orders[split]
            mask = sum(order[i] for i in range(phase) if index & (1 << i))
            got = mask | order[phase]
            for later in range(phase + 1, phases):
                gw_copy(array, split, later, got).start()

    def gw_relays(array):
        for phase in range(phases - 1):
            for index in range(1 << phase):
                gw_event(array, phase, index)

    def gw_finish(array):
        last = n_fs // 2
        wait_bytes(weights[array].at[:, pl.ds(0, last * cols)], gw_recv.at[array, last - 1])

    def r_block(array, owner, part):
        start = pl.multiple_of(owner * n + part * sub, sub)
        return rows[array].at[pl.ds(start, sub), :]

    def gz_copy(array, way, step, part):
        sign = 1 if way == 0 else -1
        there = r_block(array, tp - sign * step * CORES, part)
        return pltpu.make_async_remote_copy(
            src_ref=there,
            dst_ref=there,
            send_sem=gz_send.at[array, way],
            recv_sem=gz_recv.at[array, way, step, part],
            device_id=(fs, tp + sign * CORES),
            device_id_type=MESH,
        )

    def g_sends(way, step):
        if way == 0:
            return jnp.logical_and(z - step >= 0, z < depth - 1)
        return jnp.logical_and(z + step <= depth - 1, z > 0)

    def g_arrives(way, step):
        return z - 1 - step >= 0 if way == 0 else z + 1 + step <= depth - 1

    def gc_copy(array, way, step, part):
        sign = 1 if way == 0 else -1
        there = r_block(array, tp - sign * (step + 1) * CORES, part)
        return pltpu.make_async_remote_copy(
            src_ref=there,
            dst_ref=there,
            send_sem=gc_send.at[array],
            recv_sem=gc_recv.at[array],
            device_id=(fs, tp ^ 1),
            device_id_type=MESH,
        )

    def gz_start(array):
        for part in range(PARTS):
            for way in range(2):

                @pl.when(g_sends(way, 0))
                def _():
                    gz_copy(array, way, 0, part).start()

            gc_copy(array, 0, -1, part).start()

    def gz_event(array, step, part):
        for way in range(2):

            @pl.when(g_arrives(way, step))
            def _():
                gz_copy(array, way, step, part).wait_recv()

            if step + 1 < depth - 1:

                @pl.when(g_sends(way, step + 1))
                def _():
                    gz_copy(array, way, step + 1, part).start()

            @pl.when(g_arrives(way, step))
            def _():
                gc_copy(array, way, step, part).start()

    def gz_events(array, first, last):
        for step in range(first, last):
            for part in range(PARTS):
                gz_event(array, step, part)

    def gc_finish(array):
        wait_bytes(rows[array].at[pl.ds(0, rows_all // CORES), :], gc_recv.at[array])

    def sw_own(array, split, mask):
        return grads[array].at[pl.ds(split * half, half), slab(fs ^ mask)]

    def sw_copy(array, split, mask):
        order = orders[split]
        phase = first_bit(order, mask)
        place = compact(order, mask)
        slot, goal = place - 1, place & (place - 1)
        src = sw_own(array, split, mask) if phase == 0 else stages[array].at[split, slot // 2]
        return pltpu.make_async_remote_copy(
            src_ref=src,
            dst_ref=recvs[array].at[split, slot],
            send_sem=sw_send.at[array],
            recv_sem=sw_recv.at[array, goal // 2],
            device_id=(fs ^ order[phase], tp),
            device_id_type=MESH,
        )

    def sw_wait(array, place):
        limit = phases if place == 0 else (place & -place).bit_length() - 1
        wait_bytes(recvs[array].at[:, pl.ds(0, limit)], sw_recv.at[array, place // 2])

    def sw_sum(array, split, mask):
        order = orders[split]
        total = sw_own(array, split, mask)[...].astype(F32)
        limit = phases if mask == 0 else first_bit(order, mask)
        for phase in range(limit):
            sent = mask | order[phase]
            total += recvs[array][split, compact(order, sent) - 1].astype(F32)
        return total

    later = [m for m in range(1, n_fs) if not m & 1]
    later = sorted(later, key=lambda m: ((m & -m), -m))

    def sw_relay(array):
        for mask in later:
            sw_wait(array, mask)
            for split in range(2):
                order = orders[split]
                real = sum(bit for i, bit in enumerate(order) if mask & (1 << i))
                slot = mask - 1
                stages[array][split, slot // 2] = sw_sum(array, split, real).astype(bf16)
                sw_copy(array, split, real).start()

    def sw_finish(array):
        sw_wait(array, 0)
        for split in range(2):
            w_res[array][pl.ds(split * half, half), :] = sw_sum(array, split, 0)

    firsts = (orders[0][0], orders[1][0])
    masks = sorted(
        range(n_fs), key=lambda m: (-sum(1 for b in firsts if m & b), -m)
    )

    def weight_grad(array, left, right):
        for mask in masks:
            at = slab(fs ^ mask)
            halves = array == 2 and mask == masks[0]
            if not halves:
                grads[array][:, at] = nn(left[...], right[:, at]).astype(bf16)
            for split in range(2):
                if halves:
                    half_rows = pl.ds(split * half, half)
                    grads[array][half_rows, at] = nn(left[half_rows, :], right[:, at]).astype(bf16)
                if mask & firsts[split]:
                    sw_copy(array, split, mask).start()

    def g_rows(target, which, part):
        start = (target * CORES + which) * n + part * sub
        return pl.ds(pl.multiple_of(start, sub), sub)

    def sc_copy(target, part):
        return pltpu.make_async_remote_copy(
            src_ref=gi.at[g_rows(target, 1 - core, part), :],
            dst_ref=c_buf.at[target, part],
            send_sem=sc_send.at[0],
            recv_sem=sc_recv.at[0],
            device_id=(fs, tp ^ 1),
            device_id_type=MESH,
        )

    def sz_from(way):
        return z if way == 0 else depth - 1 - z

    def sz_target(way, step):
        return depth - 1 - step if way == 0 else step

    def sz_copy(way, step, part):
        return pltpu.make_async_remote_copy(
            src_ref=c_buf.at[sz_target(way, step), part],
            dst_ref=z_buf.at[way, step, part],
            send_sem=sz_send.at[way],
            recv_sem=sz_recv.at[way, step, part],
            device_id=(fs, tp + CORES if way == 0 else tp - CORES),
            device_id_type=MESH,
        )

    def s_sends(way, step):
        return step < depth - 1 - sz_from(way)

    targets = [depth - 1 - i // 2 if i % 2 == 0 else i // 2 for i in range(depth)]

    def sc_event(t):
        for part in range(PARTS):
            c_buf[t, part] = (
                c_buf[t, part].astype(F32) + gi[g_rows(t, core, part), :].astype(F32)
            ).astype(bf16)

    def sz_start():
        for step in range(depth - 1):
            for part in range(PARTS):
                for way in range(2):

                    @pl.when(sz_from(way) == 0)
                    def _():
                        sz_copy(way, step, part).start()

    def sz_event(hop, part):
        for way in range(2):
            step = hop - sz_from(way)

            @pl.when(jnp.logical_and(sz_from(way) > 0, step >= 0))
            def _():
                sz_copy(way, step, part).wait_recv()

                @pl.when(s_sends(way, step))
                def _():
                    t = sz_target(way, step)
                    c_buf[t, part] = (
                        c_buf[t, part].astype(F32) + z_buf[way, step, part].astype(F32)
                    ).astype(bf16)
                    sz_copy(way, step, part).start()

    def sz_finish():
        zero = jnp.zeros((sub, width), F32)
        for part in range(PARTS):
            total = c_buf[z, part].astype(F32)
            from_left = z_buf[0, jnp.clip(depth - 1 - z, 0, depth - 2), part].astype(F32)
            from_right = z_buf[1, jnp.clip(z, 0, depth - 2), part].astype(F32)
            total += jnp.where(z > 0, from_left, zero)
            total += jnp.where(z < depth - 1, from_right, zero)
            gi_res[pl.ds(part * sub, sub), :] = total.astype(bf16)

    def g_drain():
        for array in range(2):
            wait_bytes(rows[array].at[pl.ds(0, rows_all // CORES), :], gc_send.at[array])
            for way in range(2):
                for count in range(1, depth):

                    @pl.when((z if way == 0 else depth - 1 - z) == count - 1)
                    def _():
                        wait_bytes(rows[array].at[pl.ds(0, count * n), :], gz_send.at[array, way])

        for array in range(3):
            sent = weights[array].at[:, pl.ds(0, (n_fs - 1) * cols)]
            wait_bytes(sent, gw_send.at[array])

    def sz_drain():
        wait_bytes(c_buf, sc_send.at[0])
        for way in range(2):
            for count in range(1, depth):

                @pl.when(sz_from(way) == depth - 1 - count)
                def _():
                    wait_bytes(z_buf.at[way, pl.ds(0, count)], sz_send.at[way])

    def sw_drain(array):
        sent = grads[array].at[:, pl.ds(0, (n_fs - 1) * cols)]
        wait_bytes(sent, sw_send.at[array])

    tile = min(256, rows_all)

    def over_tiles(step):
        def run(i, carry):
            step(pl.ds(pl.multiple_of(i * tile, tile), tile))
            return carry

        lax.fori_loop(0, rows_all // tile, run, 0)

    def gate_step(at):
        act_buf[:, at] = nt(gate_full[...], tok_all[at, :])

    def up_step(at):
        up_pre = nt(up_full[...], tok_all[at, :])
        gate_pre = act_buf[:, at]
        sig = 1.0 / (1.0 + jnp.exp(-gate_pre))
        active = gate_pre * sig
        hid_t[:, at] = (active * up_pre).astype(bf16)
        act_buf[:, at] = active
        fac_buf[:, at] = up_pre * sig * (1.0 + gate_pre * (1.0 - sig))

    def down_step(at):
        d_hidden = nt(down_full[...], cot_all[at, :])
        d_gate = d_hidden * fac_buf[:, at]
        d_up = d_hidden * act_buf[:, at]
        dgate_t[:, at] = d_gate.astype(bf16)
        dup_t[:, at] = d_up.astype(bf16)
        dgate[at, :] = d_gate.T.astype(bf16)
        dup[at, :] = d_up.T.astype(bf16)

    gi_tile = min(512, width)

    def gi_steps(first, last):
        def run(i, carry):
            at = pl.ds(pl.multiple_of(i * gi_tile, gi_tile), gi_tile)
            gi[:, at] = (nn(dgate[...], gate_full[:, at]) + nn(dup[...], up_full[:, at])).astype(bf16)
            return carry

        lax.fori_loop(first, last, run, 0)

    TOK, COT = 0, 1
    GATE, UP, DOWN = 0, 1, 2

    gz_start(TOK)
    gw_start(GATE)
    wait_bytes(up_full.at[:, pl.ds(0, 2 * cols)], l_sem.at[2])
    local[4].wait()
    gz_event(TOK, 0, 0)
    gw_relays(GATE)
    gw_start(UP)
    for part in range(1, PARTS):
        gz_event(TOK, 0, part)
    gz_events(TOK, 1, depth - 2)
    gz_start(COT)
    gw_finish(GATE)
    gz_event(TOK, depth - 2, 0)
    gw_relays(UP)
    gw_start(DOWN)
    for part in range(1, PARTS):
        gz_event(TOK, depth - 2, part)
    gc_finish(TOK)
    over_tiles(gate_step)
    gz_events(COT, 0, 1)
    gw_finish(UP)
    over_tiles(up_step)
    gz_events(COT, 1, depth - 2)
    gw_relays(DOWN)
    gz_events(COT, depth - 2, depth - 1)
    gc_finish(COT)
    weight_grad(2, hid_t, cot_all)
    gw_finish(DOWN)
    over_tiles(down_step)
    gi_count = width // gi_tile
    gi_steps(0, gi_count // 2)
    sw_relay(2)
    gi_steps(gi_count // 2, gi_count)
    for t in targets:
        for part in range(PARTS):
            sc_copy(t, part).start()
    weight_grad(0, dgate_t, tok_all)
    wait_bytes(c_buf, sc_recv.at[0])
    for t in targets:
        sc_event(t)
    sz_start()
    weight_grad(1, dup_t, tok_all)
    g_drain()
    sw_finish(2)
    sw_drain(2)
    for hop in range(1, depth):
        for part in range(PARTS):
            sz_event(hop, part)
        if hop == 1:
            sw_relay(0)
        if hop == max(depth - 2, 1):
            sw_relay(1)
    sz_finish()
    sz_drain()
    sw_finish(0)
    sw_finish(1)

    sw_drain(0)
    sw_drain(1)


def layer(n_fs, n_tp, tokens, gate, up, down, cot):
    depth = n_tp // CORES
    n, width = tokens.shape
    ff, cols = gate.shape
    rows_all = n * n_tp
    bf16 = tokens.dtype
    hbm = pl.BlockSpec(memory_space=pl.ANY)
    vmem = pltpu.VMEM
    dma = pltpu.SemaphoreType.DMA
    half, sub = ff // 2, n // PARTS
    n_stage = max(n_fs // 2 - 1, 1)
    scratch = (
        [vmem((rows_all, width), bf16)] * 2
        + [vmem((ff, width), bf16)] * 3
        + [vmem((ff, rows_all), F32)] * 2
        + [vmem((ff, rows_all), bf16)] * 3
        + [vmem((rows_all, ff), bf16)] * 2
        + [vmem((ff, width), bf16)] * 3
        + [vmem((2, n_fs - 1, half, cols), bf16)] * 3
        + [vmem((2, n_stage, half, cols), bf16)] * 3
        + [
            vmem((rows_all, width), bf16),
            vmem((depth, PARTS, sub, width), bf16),
            vmem((2, depth - 1, PARTS, sub, width), bf16),
        ]
        + [
            dma((3,)),
            dma((3, n_fs // 2)),
            dma((2, 2)),
            dma((2, 2, depth - 1, PARTS)),
            dma((2,)),
            dma((2,)),
            dma((4,)),
            dma((3,)),
            dma((3, n_fs // 2)),
            dma((2,)),
            dma((2, depth - 1, PARTS)),
            dma((1,)),
            dma((1,)),
        ]
    )
    return pl.pallas_call(
        functools.partial(layer_kernel, n_fs, n_tp),
        out_shape=(vmem((n, width), bf16),) + (vmem((ff, cols), F32),) * 3,
        in_specs=[hbm] * 5,
        out_specs=[pl.BlockSpec(memory_space=vmem)] * 4,
        scratch_shapes=scratch,
        compiler_params=pltpu.CompilerParams(
            collective_id=0, has_side_effects=True, vmem_limit_bytes=61000000
        ),
        name="layer",
    )(tokens, gate, up, down, cot)


def deliver_kernel(*refs):
    ins, outs, sem = refs[:4], refs[4:8], refs[8]
    copies = [pltpu.make_async_copy(a, b, sem.at[i]) for i, (a, b) in enumerate(zip(ins, outs))]
    for copy in copies:
        copy.start()
    for copy in copies:
        copy.wait()


def deliver(*arrays):
    return pl.pallas_call(
        deliver_kernel,
        out_shape=tuple(jax.ShapeDtypeStruct(a.shape, a.dtype) for a in arrays),
        in_specs=[pl.BlockSpec(memory_space=pltpu.VMEM)] * 4,
        out_specs=[pl.BlockSpec(memory_space=pl.ANY)] * 4,
        scratch_shapes=[pltpu.SemaphoreType.DMA((4,))],
        compiler_params=pltpu.CompilerParams(vmem_limit_bytes=1 << 20),
        name="deliver",
    )(*arrays)


def body(n_fs, n_tp, tokens, gate_weight, up_weight, down_weight, grad_out):
    results = layer(n_fs, n_tp, tokens, gate_weight.T, up_weight.T, down_weight, grad_out)
    grad_input, grad_gate, grad_up, grad_down = deliver(*results)
    return grad_input, grad_gate.T, grad_up.T, grad_down


def solution(mesh):
    in_specs = (
        P(("fs", "tp"), None),
        P("fs", "tp"),
        P("fs", "tp"),
        P("tp", "fs"),
        P(("fs", "tp"), None),
    )
    out_specs = (P(("fs", "tp"), None), P("fs", "tp"), P("fs", "tp"), P("tp", "fs"))
    return jax.shard_map(
        functools.partial(body, mesh.shape["fs"], mesh.shape["tp"]),
        mesh=mesh,
        in_specs=in_specs,
        out_specs=out_specs,
        check_vma=False,
    )
```

```python
import functools

import jax
import jax.numpy as jnp
from jax import lax
from jax.experimental import pallas as pl
from jax.experimental.pallas import tpu as pltpu
from jax.sharding import PartitionSpec as P

MESH = pl.DeviceIdType.MESH
CORES = 2
PARTS = 2
F32 = jnp.float32


def nt(left, right):
    return lax.dot_general(left, right, (((1,), (1,)), ((), ())), preferred_element_type=F32)


def nn(left, right):
    return jnp.dot(left, right, preferred_element_type=F32)


def orders_of(n_fs):
    bits = [1 << i for i in range(n_fs.bit_length() - 1)]
    return (bits, bits[::-1])


def first_bit(order, mask):
    return next(i for i, bit in enumerate(order) if mask & bit)


def compact(order, mask):
    return sum(1 << i for i, bit in enumerate(order) if mask & bit)


def wait_bytes(ref, sem):
    pltpu.make_async_copy(ref, ref, sem).wait()


def greet(n_fs, depth, fs, tp, z):
    barrier = pltpu.get_barrier_semaphore()
    bits = orders_of(n_fs)[0]

    def hello(fs_id, tp_id):
        pl.semaphore_signal(barrier, inc=1, device_id=(fs_id, tp_id), device_id_type=MESH)

    for bit in bits:
        hello(fs ^ bit, tp)
    hello(fs, tp ^ 1)

    @pl.when(z > 0)
    def _():
        hello(fs, tp - CORES)

    @pl.when(z < depth - 1)
    def _():
        hello(fs, tp + CORES)

    ends = (z > 0).astype(jnp.int32) + (z < depth - 1).astype(jnp.int32)
    pl.semaphore_wait(barrier, len(bits) + 1 + ends)


def layer_kernel(n_fs, n_tp, *refs):
    ins, outs, scratch = refs[:5], refs[5:10], refs[10:]
    tok_all, cot_all, gate_full, up_full, down_full = scratch[:5]
    act_buf, fac_buf, hid_t, dgate_t, dup_t, dgate, dup = scratch[5:12]
    grads, recvs, stages = scratch[12:14], scratch[14:16], scratch[16:19]
    grads, recvs = (grads[0], outs[3], grads[1]), (recvs[0], outs[4], recvs[1])
    gi, c_buf, z_buf = scratch[19:22]
    gw_send, gw_recv, gz_send, gz_recv, gc_send, gc_recv, l_sem = scratch[22:29]
    sw_send, sw_recv, sz_send, sz_recv, sc_send, sc_recv = scratch[29:]
    fs, tp = lax.axis_index("fs"), lax.axis_index("tp")
    depth = n_tp // CORES
    z, core = tp // CORES, tp % CORES
    orders = orders_of(n_fs)
    phases = len(orders[0])
    bf16 = tok_all.dtype
    rows_all, width = tok_all.shape
    n = rows_all // n_tp
    ff = gate_full.shape[0]
    cols = width // n_fs
    half = ff // 2
    sub = n // PARTS
    rows = (tok_all, cot_all)
    weights = (gate_full, up_full, down_full)
    gi_res, w_res = outs[0], (outs[1], None, outs[2])

    def slab(owner):
        return pl.ds(pl.multiple_of(owner * cols, cols), cols)

    def own_rows(owner):
        return pl.ds(pl.multiple_of(owner * n, n), n)

    local = [
        pltpu.make_async_copy(ins[0], tok_all.at[own_rows(tp), :], l_sem.at[0]),
        pltpu.make_async_copy(ins[1], gate_full.at[:, slab(fs)], l_sem.at[1]),
        pltpu.make_async_copy(ins[2], up_full.at[:, slab(fs)], l_sem.at[2]),
        pltpu.make_async_copy(ins[3], down_full.at[:, slab(fs)], l_sem.at[2]),
        pltpu.make_async_copy(ins[4], cot_all.at[own_rows(tp), :], l_sem.at[3]),
    ]
    for copy in local:
        copy.start()
    greet(n_fs, depth, fs, tp, z)
    for copy in local[:2]:
        copy.wait()

    def gw_copy(array, split, phase, mask):
        order = orders[split]
        there = weights[array].at[pl.ds(split * half, half), slab(fs ^ mask)]
        slot = (1 << phase) - 1 + sum(1 << i for i in range(phase) if mask & order[i])
        return pltpu.make_async_remote_copy(
            src_ref=there,
            dst_ref=there,
            send_sem=gw_send.at[array],
            recv_sem=gw_recv.at[array, min(slot, n_fs // 2 - 1)],
            device_id=(fs ^ order[phase], tp),
            device_id_type=MESH,
        )

    def gw_start(array):
        for phase in range(phases):
            for split in range(2):
                gw_copy(array, split, phase, 0).start()

    def gw_event(array, phase, index):
        slot = (1 << phase) - 1 + index
        wait_bytes(weights[array].at[:, pl.ds(0, cols)], gw_recv.at[array, slot])
        for split in range(2):
            order = orders[split]
            mask = sum(order[i] for i in range(phase) if index & (1 << i))
            got = mask | order[phase]
            for later in range(phase + 1, phases):
                gw_copy(array, split, later, got).start()

    def gw_relays(array):
        for phase in range(phases - 1):
            for index in range(1 << phase):
                gw_event(array, phase, index)

    def gw_finish(array):
        last = n_fs // 2
        wait_bytes(weights[array].at[:, pl.ds(0, last * cols)], gw_recv.at[array, last - 1])

    def r_block(array, owner, part):
        start = pl.multiple_of(owner * n + part * sub, sub)
        return rows[array].at[pl.ds(start, sub), :]

    def gz_copy(array, way, step, part):
        sign = 1 if way == 0 else -1
        there = r_block(array, tp - sign * step * CORES, part)
        return pltpu.make_async_remote_copy(
            src_ref=there,
            dst_ref=there,
            send_sem=gz_send.at[array, way],
            recv_sem=gz_recv.at[array, way, step, part],
            device_id=(fs, tp + sign * CORES),
            device_id_type=MESH,
        )

    def g_sends(way, step):
        if way == 0:
            return jnp.logical_and(z - step >= 0, z < depth - 1)
        return jnp.logical_and(z + step <= depth - 1, z > 0)

    def g_arrives(way, step):
        return z - 1 - step >= 0 if way == 0 else z + 1 + step <= depth - 1

    def gc_copy(array, way, step, part):
        sign = 1 if way == 0 else -1
        there = r_block(array, tp - sign * (step + 1) * CORES, part)
        return pltpu.make_async_remote_copy(
            src_ref=there,
            dst_ref=there,
            send_sem=gc_send.at[array],
            recv_sem=gc_recv.at[array],
            device_id=(fs, tp ^ 1),
            device_id_type=MESH,
        )

    def gz_start(array):
        for part in range(PARTS):
            for way in range(2):

                @pl.when(g_sends(way, 0))
                def _():
                    gz_copy(array, way, 0, part).start()

            gc_copy(array, 0, -1, part).start()

    def gz_event(array, step, part):
        for way in range(2):

            @pl.when(g_arrives(way, step))
            def _():
                gz_copy(array, way, step, part).wait_recv()

            if step + 1 < depth - 1:

                @pl.when(g_sends(way, step + 1))
                def _():
                    gz_copy(array, way, step + 1, part).start()

            @pl.when(g_arrives(way, step))
            def _():
                gc_copy(array, way, step, part).start()

    def gz_events(array, first, last):
        for step in range(first, last):
            for part in range(PARTS):
                gz_event(array, step, part)

    def gc_finish(array):
        wait_bytes(rows[array].at[pl.ds(0, rows_all // CORES), :], gc_recv.at[array])

    def sw_own(array, split, mask):
        return grads[array].at[pl.ds(split * half, half), slab(fs ^ mask)]

    def sw_copy(array, split, mask):
        order = orders[split]
        phase = first_bit(order, mask)
        place = compact(order, mask)
        slot, goal = place - 1, place & (place - 1)
        src = sw_own(array, split, mask) if phase == 0 else stages[array].at[split, slot // 2]
        return pltpu.make_async_remote_copy(
            src_ref=src,
            dst_ref=recvs[array].at[split, slot],
            send_sem=sw_send.at[array],
            recv_sem=sw_recv.at[array, goal // 2],
            device_id=(fs ^ order[phase], tp),
            device_id_type=MESH,
        )

    def sw_wait(array, place):
        limit = phases if place == 0 else (place & -place).bit_length() - 1
        wait_bytes(recvs[array].at[:, pl.ds(0, limit)], sw_recv.at[array, place // 2])

    def sw_sum(array, split, mask):
        order = orders[split]
        total = sw_own(array, split, mask)[...].astype(F32)
        limit = phases if mask == 0 else first_bit(order, mask)
        for phase in range(limit):
            sent = mask | order[phase]
            total += recvs[array][split, compact(order, sent) - 1].astype(F32)
        return total

    later = [m for m in range(1, n_fs) if not m & 1]
    later = sorted(later, key=lambda m: ((m & -m), -m))

    def sw_relay(array):
        for mask in later:
            sw_wait(array, mask)
            for split in range(2):
                order = orders[split]
                real = sum(bit for i, bit in enumerate(order) if mask & (1 << i))
                slot = mask - 1
                stages[array][split, slot // 2] = sw_sum(array, split, real).astype(bf16)
                sw_copy(array, split, real).start()

    def sw_finish(array):
        sw_wait(array, 0)
        for split in range(2):
            w_res[array][pl.ds(split * half, half), :] = sw_sum(array, split, 0)

    firsts = (orders[0][0], orders[1][0])
    masks = sorted(
        range(n_fs), key=lambda m: (-sum(1 for b in firsts if m & b), -m)
    )

    def weight_grad(array, left, right):
        for mask in masks:
            at = slab(fs ^ mask)
            halves = array == 2 and mask == masks[0]
            if not halves:
                grads[array][:, at] = nn(left[...], right[:, at]).astype(bf16)
            for split in range(2):
                if halves:
                    half_rows = pl.ds(split * half, half)
                    grads[array][half_rows, at] = nn(left[half_rows, :], right[:, at]).astype(bf16)
                if mask & firsts[split]:
                    sw_copy(array, split, mask).start()

    def g_rows(target, which, part):
        start = (target * CORES + which) * n + part * sub
        return pl.ds(pl.multiple_of(start, sub), sub)

    def sc_copy(target, part):
        return pltpu.make_async_remote_copy(
            src_ref=gi.at[g_rows(target, 1 - core, part), :],
            dst_ref=c_buf.at[target, part],
            send_sem=sc_send.at[0],
            recv_sem=sc_recv.at[0],
            device_id=(fs, tp ^ 1),
            device_id_type=MESH,
        )

    def sz_from(way):
        return z if way == 0 else depth - 1 - z

    def sz_target(way, step):
        return depth - 1 - step if way == 0 else step

    def sz_copy(way, step, part):
        return pltpu.make_async_remote_copy(
            src_ref=c_buf.at[sz_target(way, step), part],
            dst_ref=z_buf.at[way, step, part],
            send_sem=sz_send.at[way],
            recv_sem=sz_recv.at[way, step, part],
            device_id=(fs, tp + CORES if way == 0 else tp - CORES),
            device_id_type=MESH,
        )

    def s_sends(way, step):
        return step < depth - 1 - sz_from(way)

    targets = [depth - 1 - i // 2 if i % 2 == 0 else i // 2 for i in range(depth)]

    def sc_event(t):
        for part in range(PARTS):
            c_buf[t, part] = (
                c_buf[t, part].astype(F32) + gi[g_rows(t, core, part), :].astype(F32)
            ).astype(bf16)

    def sz_start():
        for step in range(depth - 1):
            for part in range(PARTS):
                for way in range(2):

                    @pl.when(sz_from(way) == 0)
                    def _():
                        sz_copy(way, step, part).start()

    def sz_event(hop, part):
        for way in range(2):
            step = hop - sz_from(way)

            @pl.when(jnp.logical_and(sz_from(way) > 0, step >= 0))
            def _():
                sz_copy(way, step, part).wait_recv()

                @pl.when(s_sends(way, step))
                def _():
                    t = sz_target(way, step)
                    c_buf[t, part] = (
                        c_buf[t, part].astype(F32) + z_buf[way, step, part].astype(F32)
                    ).astype(bf16)
                    sz_copy(way, step, part).start()

    def sz_finish():
        zero = jnp.zeros((sub, width), F32)
        for part in range(PARTS):
            total = c_buf[z, part].astype(F32)
            from_left = z_buf[0, jnp.clip(depth - 1 - z, 0, depth - 2), part].astype(F32)
            from_right = z_buf[1, jnp.clip(z, 0, depth - 2), part].astype(F32)
            total += jnp.where(z > 0, from_left, zero)
            total += jnp.where(z < depth - 1, from_right, zero)
            gi_res[pl.ds(part * sub, sub), :] = total.astype(bf16)

    def g_drain():
        for array in range(2):
            wait_bytes(rows[array].at[pl.ds(0, rows_all // CORES), :], gc_send.at[array])
            for way in range(2):
                for count in range(1, depth):

                    @pl.when((z if way == 0 else depth - 1 - z) == count - 1)
                    def _():
                        wait_bytes(rows[array].at[pl.ds(0, count * n), :], gz_send.at[array, way])

        for array in range(3):
            sent = weights[array].at[:, pl.ds(0, (n_fs - 1) * cols)]
            wait_bytes(sent, gw_send.at[array])

    def sz_drain():
        wait_bytes(c_buf, sc_send.at[0])
        for way in range(2):
            for count in range(1, depth):

                @pl.when(sz_from(way) == depth - 1 - count)
                def _():
                    wait_bytes(z_buf.at[way, pl.ds(0, count)], sz_send.at[way])

    def sw_drain(array):
        sent = grads[array].at[:, pl.ds(0, (n_fs - 1) * cols)]
        wait_bytes(sent, sw_send.at[array])

    tile = min(256, rows_all)

    def over_tiles(step):
        def run(i, carry):
            step(pl.ds(pl.multiple_of(i * tile, tile), tile))
            return carry

        lax.fori_loop(0, rows_all // tile, run, 0)

    def gate_step(at):
        act_buf[:, at] = nt(gate_full[...], tok_all[at, :])

    def up_step(at):
        up_pre = nt(up_full[...], tok_all[at, :])
        gate_pre = act_buf[:, at]
        sig = 1.0 / (1.0 + jnp.exp(-gate_pre))
        active = gate_pre * sig
        hid_t[:, at] = (active * up_pre).astype(bf16)
        act_buf[:, at] = active
        fac_buf[:, at] = up_pre * sig * (1.0 + gate_pre * (1.0 - sig))

    def down_step(at):
        d_hidden = nt(down_full[...], cot_all[at, :])
        d_gate = d_hidden * fac_buf[:, at]
        d_up = d_hidden * act_buf[:, at]
        dgate_t[:, at] = d_gate.astype(bf16)
        dup_t[:, at] = d_up.astype(bf16)
        dgate[at, :] = d_gate.T.astype(bf16)
        dup[at, :] = d_up.T.astype(bf16)

    gi_tile = min(512, width)

    def gi_steps(first, last):
        def run(i, carry):
            at = pl.ds(pl.multiple_of(i * gi_tile, gi_tile), gi_tile)
            gi[:, at] = (nn(dgate[...], gate_full[:, at]) + nn(dup[...], up_full[:, at])).astype(bf16)
            return carry

        lax.fori_loop(first, last, run, 0)

    TOK, COT = 0, 1
    GATE, UP, DOWN = 0, 1, 2

    gz_start(TOK)
    gw_start(GATE)
    wait_bytes(up_full.at[:, pl.ds(0, 2 * cols)], l_sem.at[2])
    local[4].wait()
    gz_event(TOK, 0, 0)
    gw_relays(GATE)
    gw_start(UP)
    for part in range(1, PARTS):
        gz_event(TOK, 0, part)
    gz_events(TOK, 1, depth - 2)
    gz_start(COT)
    gw_finish(GATE)
    gz_event(TOK, depth - 2, 0)
    gw_relays(UP)
    gw_start(DOWN)
    for part in range(1, PARTS):
        gz_event(TOK, depth - 2, part)
    gc_finish(TOK)
    over_tiles(gate_step)
    gz_events(COT, 0, 1)
    gw_finish(UP)
    over_tiles(up_step)
    gz_events(COT, 1, depth - 2)
    gw_relays(DOWN)
    gz_events(COT, depth - 2, depth - 1)
    gc_finish(COT)
    weight_grad(2, hid_t, cot_all)
    gw_finish(DOWN)
    over_tiles(down_step)
    gi_count = width // gi_tile
    gi_steps(0, gi_count // 2)
    sw_relay(2)
    gi_steps(gi_count // 2, gi_count)
    for t in targets:
        for part in range(PARTS):
            sc_copy(t, part).start()
    weight_grad(0, dgate_t, tok_all)
    wait_bytes(c_buf, sc_recv.at[0])
    for t in targets:
        sc_event(t)
    sz_start()
    weight_grad(1, dup_t, tok_all)
    g_drain()
    sw_finish(2)
    sw_drain(2)
    for hop in range(1, depth):
        for part in range(PARTS):
            sz_event(hop, part)
        if hop == 1:
            sw_relay(0)
        if hop == max(depth - 2, 1):
            sw_relay(1)
    sz_finish()
    sz_drain()
    sw_finish(0)
    sw_wait(1, 0)

    sw_drain(0)
    sw_drain(1)


def layer(n_fs, n_tp, tokens, gate, up, down, cot):
    depth = n_tp // CORES
    n, width = tokens.shape
    ff, cols = gate.shape
    rows_all = n * n_tp
    bf16 = tokens.dtype
    hbm = pl.BlockSpec(memory_space=pl.ANY)
    vmem = pltpu.VMEM
    dma = pltpu.SemaphoreType.DMA
    half, sub = ff // 2, n // PARTS
    n_stage = max(n_fs // 2 - 1, 1)
    scratch = (
        [vmem((rows_all, width), bf16)] * 2
        + [vmem((ff, width), bf16)] * 3
        + [vmem((ff, rows_all), F32)] * 2
        + [vmem((ff, rows_all), bf16)] * 3
        + [vmem((rows_all, ff), bf16)] * 2
        + [vmem((ff, width), bf16)] * 2
        + [vmem((2, n_fs - 1, half, cols), bf16)] * 2
        + [vmem((2, n_stage, half, cols), bf16)] * 3
        + [
            vmem((rows_all, width), bf16),
            vmem((depth, PARTS, sub, width), bf16),
            vmem((2, depth - 1, PARTS, sub, width), bf16),
        ]
        + [
            dma((3,)),
            dma((3, n_fs // 2)),
            dma((2, 2)),
            dma((2, 2, depth - 1, PARTS)),
            dma((2,)),
            dma((2,)),
            dma((4,)),
            dma((3,)),
            dma((3, n_fs // 2)),
            dma((2,)),
            dma((2, depth - 1, PARTS)),
            dma((1,)),
            dma((1,)),
        ]
    )
    return pl.pallas_call(
        functools.partial(layer_kernel, n_fs, n_tp),
        out_shape=(vmem((n, width), bf16),)
        + (vmem((ff, cols), F32),) * 2
        + (vmem((ff, width), bf16), vmem((2, n_fs - 1, half, cols), bf16)),
        in_specs=[hbm] * 5,
        out_specs=[pl.BlockSpec(memory_space=vmem)] * 5,
        scratch_shapes=scratch,
        compiler_params=pltpu.CompilerParams(
            collective_id=0, has_side_effects=True, vmem_limit_bytes=57000000
        ),
        name="layer",
    )(tokens, gate, up, down, cot)


def deliver_kernel(n_fs, *refs):
    gi, gate, down, own, got = refs[:5]
    outs, total, sem = refs[5:9], refs[9], refs[10]
    half, cols = got.shape[2:]
    fs = lax.axis_index("fs")
    slab = pl.ds(pl.multiple_of(fs * cols, cols), cols)
    copies = [
        pltpu.make_async_copy(a, outs[i], sem.at[i]) for a, i in ((gi, 0), (gate, 1), (down, 3))
    ]
    for copy in copies:
        copy.start()
    for split in range(2):
        at = pl.ds(split * half, half)
        summed = own[at, slab].astype(F32)
        for phase in range(n_fs.bit_length() - 1):
            summed += got[split, (1 << phase) - 1].astype(F32)
        total[at, :] = summed
        copies.append(pltpu.make_async_copy(total.at[at, :], outs[2].at[at, :], sem.at[4 + split]))
        copies[-1].start()
    for copy in copies:
        copy.wait()


def deliver(n_fs, gi, gate, down, own, got):
    vmem = pltpu.VMEM
    shapes = [jax.ShapeDtypeStruct(a.shape, a.dtype) for a in (gi, gate, gate, down)]
    return pl.pallas_call(
        functools.partial(deliver_kernel, n_fs),
        out_shape=tuple(shapes),
        in_specs=[pl.BlockSpec(memory_space=vmem)] * 5,
        out_specs=[pl.BlockSpec(memory_space=pl.ANY)] * 4,
        scratch_shapes=[vmem(gate.shape, F32), pltpu.SemaphoreType.DMA((6,))],
        compiler_params=pltpu.CompilerParams(vmem_limit_bytes=2 << 20),
        name="deliver",
    )(gi, gate, down, own, got)


def body(n_fs, n_tp, tokens, gate_weight, up_weight, down_weight, grad_out):
    results = layer(n_fs, n_tp, tokens, gate_weight.T, up_weight.T, down_weight, grad_out)
    grad_input, grad_gate, grad_up, grad_down = deliver(n_fs, *results)
    return grad_input, grad_gate.T, grad_up.T, grad_down


def solution(mesh):
    in_specs = (
        P(("fs", "tp"), None),
        P("fs", "tp"),
        P("fs", "tp"),
        P("tp", "fs"),
        P(("fs", "tp"), None),
    )
    out_specs = (P(("fs", "tp"), None), P("fs", "tp"), P("fs", "tp"), P("tp", "fs"))
    return jax.shard_map(
        functools.partial(body, mesh.shape["fs"], mesh.shape["tp"]),
        mesh=mesh,
        in_specs=in_specs,
        out_specs=out_specs,
        check_vma=False,
    )
```

```python
import functools

import jax
import jax.numpy as jnp
from jax import lax
from jax.experimental import pallas as pl
from jax.experimental.pallas import tpu as pltpu
from jax.sharding import PartitionSpec as P

MESH = pl.DeviceIdType.MESH
CORES = 2
PARTS = 2
SUM_PARTS = 1
F32 = jnp.float32


def nt(left, right):
    return lax.dot_general(left, right, (((1,), (1,)), ((), ())), preferred_element_type=F32)


def nn(left, right):
    return jnp.dot(left, right, preferred_element_type=F32)


def orders_of(n_fs):
    bits = [1 << i for i in range(n_fs.bit_length() - 1)]
    return (bits, bits[::-1])


def first_bit(order, mask):
    return next(i for i, bit in enumerate(order) if mask & bit)


def compact(order, mask):
    return sum(1 << i for i, bit in enumerate(order) if mask & bit)


def wait_bytes(ref, sem):
    pltpu.make_async_copy(ref, ref, sem).wait()


def greet(n_fs, depth, fs, tp, z):
    barrier = pltpu.get_barrier_semaphore()
    bits = orders_of(n_fs)[0]

    def hello(fs_id, tp_id):
        pl.semaphore_signal(barrier, inc=1, device_id=(fs_id, tp_id), device_id_type=MESH)

    for bit in bits:
        hello(fs ^ bit, tp)
    hello(fs, tp ^ 1)

    @pl.when(z > 0)
    def _():
        hello(fs, tp - CORES)

    @pl.when(z < depth - 1)
    def _():
        hello(fs, tp + CORES)

    ends = (z > 0).astype(jnp.int32) + (z < depth - 1).astype(jnp.int32)
    pl.semaphore_wait(barrier, len(bits) + 1 + ends)


def layer_kernel(n_fs, n_tp, *refs):
    ins, outs, scratch = refs[:5], refs[5:10], refs[10:]
    tok_all, cot_all, gate_full, up_full, down_full = scratch[:5]
    act_buf, fac_buf, hid_t, dgate_t, dup_t, dgate, dup = scratch[5:12]
    grads, recvs, stages = scratch[12:14], scratch[14:16], scratch[16:19]
    grads, recvs = (grads[0], outs[3], grads[1]), (recvs[0], outs[4], recvs[1])
    gi, c_buf, z_buf = scratch[19:22]
    gw_send, gw_recv, gz_send, gz_recv, gc_send, gc_recv, l_sem = scratch[22:29]
    sw_send, sw_recv, sz_send, sz_recv, sc_send, sc_recv = scratch[29:]
    fs, tp = lax.axis_index("fs"), lax.axis_index("tp")
    depth = n_tp // CORES
    z, core = tp // CORES, tp % CORES
    orders = orders_of(n_fs)
    phases = len(orders[0])
    bf16 = tok_all.dtype
    rows_all, width = tok_all.shape
    n = rows_all // n_tp
    ff = gate_full.shape[0]
    cols = width // n_fs
    half = ff // 2
    sub = n // PARTS
    piece = n // SUM_PARTS
    rows = (tok_all, cot_all)
    weights = (gate_full, up_full, down_full)
    gi_res, w_res = outs[0], (outs[1], None, outs[2])

    def slab(owner):
        return pl.ds(pl.multiple_of(owner * cols, cols), cols)

    def own_rows(owner):
        return pl.ds(pl.multiple_of(owner * n, n), n)

    local = [
        pltpu.make_async_copy(ins[0], tok_all.at[own_rows(tp), :], l_sem.at[0]),
        pltpu.make_async_copy(ins[1], gate_full.at[:, slab(fs)], l_sem.at[1]),
        pltpu.make_async_copy(ins[2], up_full.at[:, slab(fs)], l_sem.at[2]),
        pltpu.make_async_copy(ins[3], down_full.at[:, slab(fs)], l_sem.at[2]),
        pltpu.make_async_copy(ins[4], cot_all.at[own_rows(tp), :], l_sem.at[3]),
    ]
    for copy in local:
        copy.start()
    greet(n_fs, depth, fs, tp, z)
    for copy in local[:2]:
        copy.wait()

    def gw_copy(array, split, phase, mask):
        order = orders[split]
        there = weights[array].at[pl.ds(split * half, half), slab(fs ^ mask)]
        slot = (1 << phase) - 1 + sum(1 << i for i in range(phase) if mask & order[i])
        return pltpu.make_async_remote_copy(
            src_ref=there,
            dst_ref=there,
            send_sem=gw_send.at[array],
            recv_sem=gw_recv.at[array, min(slot, n_fs // 2 - 1)],
            device_id=(fs ^ order[phase], tp),
            device_id_type=MESH,
        )

    def gw_start(array):
        for phase in range(phases):
            for split in range(2):
                gw_copy(array, split, phase, 0).start()

    def gw_event(array, phase, index):
        slot = (1 << phase) - 1 + index
        wait_bytes(weights[array].at[:, pl.ds(0, cols)], gw_recv.at[array, slot])
        for split in range(2):
            order = orders[split]
            mask = sum(order[i] for i in range(phase) if index & (1 << i))
            got = mask | order[phase]
            for later in range(phase + 1, phases):
                gw_copy(array, split, later, got).start()

    def gw_relays(array):
        for phase in range(phases - 1):
            for index in range(1 << phase):
                gw_event(array, phase, index)

    def gw_finish(array):
        last = n_fs // 2
        wait_bytes(weights[array].at[:, pl.ds(0, last * cols)], gw_recv.at[array, last - 1])

    def r_block(array, owner, part):
        start = pl.multiple_of(owner * n + part * sub, sub)
        return rows[array].at[pl.ds(start, sub), :]

    def gz_copy(array, way, step, part):
        sign = 1 if way == 0 else -1
        there = r_block(array, tp - sign * step * CORES, part)
        return pltpu.make_async_remote_copy(
            src_ref=there,
            dst_ref=there,
            send_sem=gz_send.at[array, way],
            recv_sem=gz_recv.at[array, way, step, part],
            device_id=(fs, tp + sign * CORES),
            device_id_type=MESH,
        )

    def g_sends(way, step):
        if way == 0:
            return jnp.logical_and(z - step >= 0, z < depth - 1)
        return jnp.logical_and(z + step <= depth - 1, z > 0)

    def g_arrives(way, step):
        return z - 1 - step >= 0 if way == 0 else z + 1 + step <= depth - 1

    def gc_copy(array, way, step, part):
        sign = 1 if way == 0 else -1
        there = r_block(array, tp - sign * (step + 1) * CORES, part)
        return pltpu.make_async_remote_copy(
            src_ref=there,
            dst_ref=there,
            send_sem=gc_send.at[array],
            recv_sem=gc_recv.at[array],
            device_id=(fs, tp ^ 1),
            device_id_type=MESH,
        )

    def gz_start(array):
        for part in range(PARTS):
            for way in range(2):

                @pl.when(g_sends(way, 0))
                def _():
                    gz_copy(array, way, 0, part).start()

            gc_copy(array, 0, -1, part).start()

    def gz_event(array, step, part):
        for way in range(2):

            @pl.when(g_arrives(way, step))
            def _():
                gz_copy(array, way, step, part).wait_recv()

            if step + 1 < depth - 1:

                @pl.when(g_sends(way, step + 1))
                def _():
                    gz_copy(array, way, step + 1, part).start()

            @pl.when(g_arrives(way, step))
            def _():
                gc_copy(array, way, step, part).start()

    def gz_events(array, first, last):
        for step in range(first, last):
            for part in range(PARTS):
                gz_event(array, step, part)

    def gc_finish(array):
        wait_bytes(rows[array].at[pl.ds(0, rows_all // CORES), :], gc_recv.at[array])

    def sw_own(array, split, mask):
        return grads[array].at[pl.ds(split * half, half), slab(fs ^ mask)]

    def sw_copy(array, split, mask):
        order = orders[split]
        phase = first_bit(order, mask)
        place = compact(order, mask)
        slot, goal = place - 1, place & (place - 1)
        src = sw_own(array, split, mask) if phase == 0 else stages[array].at[split, slot // 2]
        return pltpu.make_async_remote_copy(
            src_ref=src,
            dst_ref=recvs[array].at[split, slot],
            send_sem=sw_send.at[array],
            recv_sem=sw_recv.at[array, goal // 2],
            device_id=(fs ^ order[phase], tp),
            device_id_type=MESH,
        )

    def sw_wait(array, place):
        limit = phases if place == 0 else (place & -place).bit_length() - 1
        wait_bytes(recvs[array].at[:, pl.ds(0, limit)], sw_recv.at[array, place // 2])

    def sw_sum(array, split, mask):
        order = orders[split]
        total = sw_own(array, split, mask)[...].astype(F32)
        limit = phases if mask == 0 else first_bit(order, mask)
        for phase in range(limit):
            sent = mask | order[phase]
            total += recvs[array][split, compact(order, sent) - 1].astype(F32)
        return total

    later = [m for m in range(1, n_fs) if not m & 1]
    later = sorted(later, key=lambda m: ((m & -m), -m))

    def sw_relay(array):
        for mask in later:
            sw_wait(array, mask)
            for split in range(2):
                order = orders[split]
                real = sum(bit for i, bit in enumerate(order) if mask & (1 << i))
                slot = mask - 1
                stages[array][split, slot // 2] = sw_sum(array, split, real).astype(bf16)
                sw_copy(array, split, real).start()

    def sw_finish(array):
        sw_wait(array, 0)
        for split in range(2):
            w_res[array][pl.ds(split * half, half), :] = sw_sum(array, split, 0)

    firsts = (orders[0][0], orders[1][0])
    masks = sorted(
        range(n_fs), key=lambda m: (-sum(1 for b in firsts if m & b), -m)
    )

    def weight_grad(array, left, right):
        for mask in masks:
            at = slab(fs ^ mask)
            halves = array == 2 and mask == masks[0]
            if not halves:
                grads[array][:, at] = nn(left[...], right[:, at]).astype(bf16)
            for split in range(2):
                if halves:
                    half_rows = pl.ds(split * half, half)
                    grads[array][half_rows, at] = nn(left[half_rows, :], right[:, at]).astype(bf16)
                if mask & firsts[split]:
                    sw_copy(array, split, mask).start()

    def g_rows(target, which, part):
        start = (target * CORES + which) * n + part * piece
        return pl.ds(pl.multiple_of(start, piece), piece)

    def sc_copy(target, part):
        return pltpu.make_async_remote_copy(
            src_ref=gi.at[g_rows(target, 1 - core, part), :],
            dst_ref=c_buf.at[target, part],
            send_sem=sc_send.at[0],
            recv_sem=sc_recv.at[0],
            device_id=(fs, tp ^ 1),
            device_id_type=MESH,
        )

    def sz_from(way):
        return z if way == 0 else depth - 1 - z

    def sz_target(way, step):
        return depth - 1 - step if way == 0 else step

    def sz_copy(way, step, part):
        return pltpu.make_async_remote_copy(
            src_ref=c_buf.at[sz_target(way, step), part],
            dst_ref=z_buf.at[way, step, part],
            send_sem=sz_send.at[way],
            recv_sem=sz_recv.at[way, step, part],
            device_id=(fs, tp + CORES if way == 0 else tp - CORES),
            device_id_type=MESH,
        )

    def s_sends(way, step):
        return step < depth - 1 - sz_from(way)

    targets = [depth - 1 - i // 2 if i % 2 == 0 else i // 2 for i in range(depth)]

    def sc_event(t):
        for part in range(SUM_PARTS):
            c_buf[t, part] = (
                c_buf[t, part].astype(F32) + gi[g_rows(t, core, part), :].astype(F32)
            ).astype(bf16)

    def sz_start():
        for step in range(depth - 1):
            for part in range(SUM_PARTS):
                for way in range(2):

                    @pl.when(sz_from(way) == 0)
                    def _():
                        sz_copy(way, step, part).start()

    def sz_event(hop, part):
        for way in range(2):
            step = hop - sz_from(way)

            @pl.when(jnp.logical_and(sz_from(way) > 0, step >= 0))
            def _():
                sz_copy(way, step, part).wait_recv()

                @pl.when(s_sends(way, step))
                def _():
                    t = sz_target(way, step)
                    c_buf[t, part] = (
                        c_buf[t, part].astype(F32) + z_buf[way, step, part].astype(F32)
                    ).astype(bf16)
                    sz_copy(way, step, part).start()

    def sz_finish():
        zero = jnp.zeros((piece, width), F32)
        for part in range(SUM_PARTS):
            total = c_buf[z, part].astype(F32)
            from_left = z_buf[0, jnp.clip(depth - 1 - z, 0, depth - 2), part].astype(F32)
            from_right = z_buf[1, jnp.clip(z, 0, depth - 2), part].astype(F32)
            total += jnp.where(z > 0, from_left, zero)
            total += jnp.where(z < depth - 1, from_right, zero)
            gi_res[pl.ds(part * piece, piece), :] = total.astype(bf16)

    def g_drain():
        for array in range(2):
            wait_bytes(rows[array].at[pl.ds(0, rows_all // CORES), :], gc_send.at[array])
            for way in range(2):
                for count in range(1, depth):

                    @pl.when((z if way == 0 else depth - 1 - z) == count - 1)
                    def _():
                        wait_bytes(rows[array].at[pl.ds(0, count * n), :], gz_send.at[array, way])

        for array in range(3):
            sent = weights[array].at[:, pl.ds(0, (n_fs - 1) * cols)]
            wait_bytes(sent, gw_send.at[array])

    def sz_drain():
        wait_bytes(c_buf, sc_send.at[0])
        for way in range(2):
            for count in range(1, depth):

                @pl.when(sz_from(way) == depth - 1 - count)
                def _():
                    wait_bytes(z_buf.at[way, pl.ds(0, count)], sz_send.at[way])

    def sw_drain(array):
        sent = grads[array].at[:, pl.ds(0, (n_fs - 1) * cols)]
        wait_bytes(sent, sw_send.at[array])

    tile = min(256, rows_all)

    def over_tiles(step):
        def run(i, carry):
            step(pl.ds(pl.multiple_of(i * tile, tile), tile))
            return carry

        lax.fori_loop(0, rows_all // tile, run, 0)

    def gate_step(at):
        act_buf[:, at] = nt(gate_full[...], tok_all[at, :])

    def up_step(at):
        up_pre = nt(up_full[...], tok_all[at, :])
        gate_pre = act_buf[:, at]
        sig = 1.0 / (1.0 + jnp.exp(-gate_pre))
        active = gate_pre * sig
        hid_t[:, at] = (active * up_pre).astype(bf16)
        act_buf[:, at] = active
        fac_buf[:, at] = up_pre * sig * (1.0 + gate_pre * (1.0 - sig))

    def down_step(at):
        d_hidden = nt(down_full[...], cot_all[at, :])
        d_gate = d_hidden * fac_buf[:, at]
        d_up = d_hidden * act_buf[:, at]
        dgate_t[:, at] = d_gate.astype(bf16)
        dup_t[:, at] = d_up.astype(bf16)
        dgate[at, :] = d_gate.T.astype(bf16)
        dup[at, :] = d_up.T.astype(bf16)

    gi_tile = min(512, width)

    def gi_steps(first, last):
        def run(i, carry):
            at = pl.ds(pl.multiple_of(i * gi_tile, gi_tile), gi_tile)
            gi[:, at] = (nn(dgate[...], gate_full[:, at]) + nn(dup[...], up_full[:, at])).astype(bf16)
            return carry

        lax.fori_loop(first, last, run, 0)

    TOK, COT = 0, 1
    GATE, UP, DOWN = 0, 1, 2

    gz_start(TOK)
    gw_start(GATE)
    wait_bytes(up_full.at[:, pl.ds(0, 2 * cols)], l_sem.at[2])
    local[4].wait()
    gz_event(TOK, 0, 0)
    gw_relays(GATE)
    gw_start(UP)
    for part in range(1, PARTS):
        gz_event(TOK, 0, part)
    gz_events(TOK, 1, depth - 2)
    gz_start(COT)
    gw_finish(GATE)
    gz_event(TOK, depth - 2, 0)
    gw_relays(UP)
    gw_start(DOWN)
    for part in range(1, PARTS):
        gz_event(TOK, depth - 2, part)
    gc_finish(TOK)
    over_tiles(gate_step)
    gz_events(COT, 0, 1)
    gw_finish(UP)
    over_tiles(up_step)
    gz_events(COT, 1, depth - 2)
    gw_relays(DOWN)
    gz_events(COT, depth - 2, depth - 1)
    gc_finish(COT)
    weight_grad(2, hid_t, cot_all)
    gw_finish(DOWN)
    over_tiles(down_step)
    gi_count = width // gi_tile
    gi_steps(0, gi_count // 2)
    sw_relay(2)
    gi_steps(gi_count // 2, gi_count)
    for t in targets:
        for part in range(SUM_PARTS):
            sc_copy(t, part).start()
    weight_grad(0, dgate_t, tok_all)
    wait_bytes(c_buf, sc_recv.at[0])
    for t in targets:
        sc_event(t)
    sz_start()
    weight_grad(1, dup_t, tok_all)
    g_drain()
    sw_finish(2)
    sw_drain(2)
    for hop in range(1, depth):
        for part in range(SUM_PARTS):
            sz_event(hop, part)
        if hop == 1:
            sw_relay(0)
        if hop == max(depth - 2, 1):
            sw_relay(1)
    sz_finish()
    sz_drain()
    sw_finish(0)
    sw_wait(1, 0)

    sw_drain(0)
    sw_drain(1)


def layer(n_fs, n_tp, tokens, gate, up, down, cot):
    depth = n_tp // CORES
    n, width = tokens.shape
    ff, cols = gate.shape
    rows_all = n * n_tp
    bf16 = tokens.dtype
    hbm = pl.BlockSpec(memory_space=pl.ANY)
    vmem = pltpu.VMEM
    dma = pltpu.SemaphoreType.DMA
    half = ff // 2
    n_stage = max(n_fs // 2 - 1, 1)
    scratch = (
        [vmem((rows_all, width), bf16)] * 2
        + [vmem((ff, width), bf16)] * 3
        + [vmem((ff, rows_all), F32)] * 2
        + [vmem((ff, rows_all), bf16)] * 3
        + [vmem((rows_all, ff), bf16)] * 2
        + [vmem((ff, width), bf16)] * 2
        + [vmem((2, n_fs - 1, half, cols), bf16)] * 2
        + [vmem((2, n_stage, half, cols), bf16)] * 3
        + [
            vmem((rows_all, width), bf16),
            vmem((depth, SUM_PARTS, n // SUM_PARTS, width), bf16),
            vmem((2, depth - 1, SUM_PARTS, n // SUM_PARTS, width), bf16),
        ]
        + [
            dma((3,)),
            dma((3, n_fs // 2)),
            dma((2, 2)),
            dma((2, 2, depth - 1, PARTS)),
            dma((2,)),
            dma((2,)),
            dma((4,)),
            dma((3,)),
            dma((3, n_fs // 2)),
            dma((2,)),
            dma((2, depth - 1, SUM_PARTS)),
            dma((1,)),
            dma((1,)),
        ]
    )
    return pl.pallas_call(
        functools.partial(layer_kernel, n_fs, n_tp),
        out_shape=(vmem((n, width), bf16),)
        + (vmem((ff, cols), F32),) * 2
        + (vmem((ff, width), bf16), vmem((2, n_fs - 1, half, cols), bf16)),
        in_specs=[hbm] * 5,
        out_specs=[pl.BlockSpec(memory_space=vmem)] * 5,
        scratch_shapes=scratch,
        compiler_params=pltpu.CompilerParams(
            collective_id=0, has_side_effects=True, vmem_limit_bytes=57000000
        ),
        name="layer",
    )(tokens, gate, up, down, cot)


def deliver_kernel(n_fs, *refs):
    gi, gate, down, own, got = refs[:5]
    outs, total, sem = refs[5:9], refs[9], refs[10]
    half, cols = got.shape[2:]
    fs = lax.axis_index("fs")
    slab = pl.ds(pl.multiple_of(fs * cols, cols), cols)
    copies = [
        pltpu.make_async_copy(a, outs[i], sem.at[i]) for a, i in ((gi, 0), (gate, 1), (down, 3))
    ]
    for copy in copies:
        copy.start()
    for split in range(2):
        at = pl.ds(split * half, half)
        summed = own[at, slab].astype(F32)
        for phase in range(n_fs.bit_length() - 1):
            summed += got[split, (1 << phase) - 1].astype(F32)
        total[at, :] = summed
        copies.append(pltpu.make_async_copy(total.at[at, :], outs[2].at[at, :], sem.at[4 + split]))
        copies[-1].start()
    for copy in copies:
        copy.wait()


def deliver(n_fs, gi, gate, down, own, got):
    vmem = pltpu.VMEM
    shapes = [jax.ShapeDtypeStruct(a.shape, a.dtype) for a in (gi, gate, gate, down)]
    return pl.pallas_call(
        functools.partial(deliver_kernel, n_fs),
        out_shape=tuple(shapes),
        in_specs=[pl.BlockSpec(memory_space=vmem)] * 5,
        out_specs=[pl.BlockSpec(memory_space=pl.ANY)] * 4,
        scratch_shapes=[vmem(gate.shape, F32), pltpu.SemaphoreType.DMA((6,))],
        compiler_params=pltpu.CompilerParams(vmem_limit_bytes=2 << 20),
        name="deliver",
    )(gi, gate, down, own, got)


def body(n_fs, n_tp, tokens, gate_weight, up_weight, down_weight, grad_out):
    results = layer(n_fs, n_tp, tokens, gate_weight.T, up_weight.T, down_weight, grad_out)
    grad_input, grad_gate, grad_up, grad_down = deliver(n_fs, *results)
    return grad_input, grad_gate.T, grad_up.T, grad_down


def solution(mesh):
    in_specs = (
        P(("fs", "tp"), None),
        P("fs", "tp"),
        P("fs", "tp"),
        P("tp", "fs"),
        P(("fs", "tp"), None),
    )
    out_specs = (P(("fs", "tp"), None), P("fs", "tp"), P("fs", "tp"), P("tp", "fs"))
    return jax.shard_map(
        functools.partial(body, mesh.shape["fs"], mesh.shape["tp"]),
        mesh=mesh,
        in_specs=in_specs,
        out_specs=out_specs,
        check_vma=False,
    )
```
